32 devices in a mesh: dp: 4 (over y, x), kv: 4 (over z), tp: 2 (over core).
Axes of the slice: x: 2, y: 2, z: 4, core: 2. Of those that a mesh axis runs over, the one named last changes fastest.
Arguments:
- tokens: bfloat16 [4096, 4096], P(('dp', 'kv')), parts along dimension 0, may hold values from -16 to 16
- query_weight: bfloat16 [4096, 1024], P('kv', 'tp'), may hold values from -0.09375 to 0.09375
- key_weight: bfloat16 [4096, 256], P('kv', 'tp'), may hold values from -0.09375 to 0.09375
- value_weight: bfloat16 [4096, 256], P('kv', 'tp'), may hold values from -0.09375 to 0.09375
- out_weight: bfloat16 [1024, 4096], P('kv', 'tp'), may hold values from -1.5 to 1.5
- chosen: int32 [128, 16], P(('dp', 'kv')), parts along dimension 0, may hold values from -1 to 31, as said below
- live_length: int32 [4], P('dp'), parts along dimension 0, may hold values from 128 to 1024
Outputs:
- mixed: bfloat16 [4096, 4096], P(('dp', 'kv'), 'tp'), parts along dimension 0
The draws below stay inside these ranges and needn't reach their ends.
There are 4 independent parts, one for each index of `dp`. The reference program is written for one: setup_inputs(seed, part) draws one part's arguments, and reference() takes and returns one part's arrays. A program takes and returns all parts, laid end to end along the dimension named above; an argument that names none is the same for every part. Nothing has to cross between parts.
Inputs may be any that keep to these rules, and one draw needn't show every extreme that they name: `chosen`: row j lists 16 entries: entry 0 is j itself, the others are distinct blocks before j, or -1 for unused entries. The query blocks of one device together read at most 2 distinct blocks held by any one other device, and some device reads 2 of another's in every draw.
All inputs are finite; a program needn't handle non-finite values.
Results may differ from the reference program's by a relative error of at most 0.0085.
Values may be sent and summed in bfloat16 or wider, within the bound.
A program may use at most 64 MiB of HBM per device.

```python
import jax
import jax.numpy as jnp
from jax import lax

D = 4096
HEADS = 8
KV_HEADS = 2
HD = 128
BLOCK = 32
NSEL = 16
CAP = 2
TOK_DEV = 256
TOKENS = 1024
SEGMENT_TOTAL = 32
Q_WIDTH = 1024
KV_WIDTH = 256
N_KV = 4


def draw_tokens(key, part):
    normal_draw = jax.random.normal(key, (TOKENS, D), jnp.float32)
    return jnp.clip(normal_draw, -6.0, 6.0).astype(jnp.bfloat16)


def draw_chosen(key, part):
    owners = TOKENS // TOK_DEV
    per_dev = TOK_DEV // BLOCK
    pick_key = jax.random.fold_in(key, 11)
    noise_key = jax.random.fold_in(key, 13)
    pick_scores = jax.random.randint(pick_key, (owners, owners, per_dev), 0, 1 << 20)
    local_ids = jnp.arange(per_dev, dtype=jnp.int32)
    order = jnp.argsort(pick_scores * per_dev + local_ids[None, None, :], axis=-1, stable=True)
    allowed_local = order[..., :CAP]
    allowed = jnp.any(local_ids[None, None, None, :] == allowed_local[..., None], axis=2)
    allowed = allowed.reshape(owners, SEGMENT_TOTAL)
    stream_segments = jnp.arange(SEGMENT_TOTAL, dtype=jnp.int32)
    segment_loader = stream_segments // per_dev
    segment_retainer = stream_segments // per_dev
    remote_segment = allowed[segment_loader] & (segment_retainer[None, :] < segment_loader[:, None])
    local = (segment_retainer[None, :] == segment_loader[:, None]) & (stream_segments[None, :] < stream_segments[:, None])
    eligible_filter = remote_segment | local
    rating_increment = jnp.where(remote_segment & (segment_retainer[None, :] == 0), 2, jnp.where(remote_segment & (segment_retainer[None, :] == segment_loader[:, None] - 1), 1, 0))
    stochastic_perturbation = jax.random.randint(noise_key, (SEGMENT_TOTAL, SEGMENT_TOTAL), 0, 1 << 12)
    segment_rating = jnp.where(eligible_filter, (stochastic_perturbation + rating_increment * (1 << 12)) * SEGMENT_TOTAL + stream_segments[None, :], -1)
    values, indices = lax.top_k(segment_rating, NSEL - 1)
    picks = jnp.where(values >= 0, indices, -1).astype(jnp.int32)
    return jnp.concatenate([stream_segments[:, None], picks], axis=1).astype(jnp.int32)


def level_of(rng, shape, split, least, high):
    def one(axis_at, parts):
        draws = jax.random.uniform(jax.random.fold_in(jax.random.fold_in(rng, 6), axis_at), (parts,), jnp.float32, least / len(split), high / len(split))
        return jnp.repeat(jnp.exp(draws), shape[axis_at] // parts).reshape((-1,) + (1,) * (len(shape) - axis_at - 1))

    loudness = one(*split[0])
    for cut in split[1:]:
        loudness = loudness * one(*cut)
    return loudness


def scatter_about(key, extent, width, bound, split=(), held_as=jnp.bfloat16):
    values = jax.random.normal(key, extent, jnp.float32) * width
    if len(split) > 0:
        values = level_of(key, extent, split, -0.22, 0.18) * values
    return jnp.clip(values, min=-bound, max=bound).astype(held_as)


def setup_inputs(seed: int = 0, part: int = 0) -> dict:
    key_list = jax.random.split(jax.random.key(seed), 8)
    part_splits = jax.random.split(jax.random.fold_in(key_list[7], part), 8)
    return {
        "tokens": draw_tokens(jax.random.fold_in(jax.random.fold_in(key_list[7], part), 71), part),
        "query_weight": scatter_about(key_list[1], (D, Q_WIDTH), D ** -0.5, 0.09375, ((0, 4), (1, 2))),
        "key_weight": scatter_about(key_list[2], (D, KV_WIDTH), D ** -0.5, 0.09375, ((0, 4), (1, 2))),
        "value_weight": scatter_about(key_list[3], (D, KV_WIDTH), D ** -0.5, 0.09375, ((0, 4), (1, 2))),
        "out_weight": scatter_about(key_list[4], (Q_WIDTH, D), (Q_WIDTH // 64) ** -0.5, 1.5, ((0, 4), (1, 2))),
        "chosen": draw_chosen(jax.random.fold_in(jax.random.fold_in(key_list[7], part), 71), part),
        "live_length": jax.random.randint(part_splits[6], (1,), TOKENS // 8, TOKENS + 1).astype(jnp.int32),
    }


def reference(tokens, query_weight, key_weight, value_weight, out_weight, chosen, live_length):
    queries = jnp.dot(tokens, query_weight, preferred_element_type=jnp.float32).astype(jnp.bfloat16)
    keys = jnp.dot(tokens, key_weight, preferred_element_type=jnp.float32).astype(jnp.bfloat16)
    values = jnp.dot(tokens, value_weight, preferred_element_type=jnp.float32).astype(jnp.bfloat16)
    groups = HEADS // KV_HEADS
    per_dev = TOK_DEV // BLOCK
    key_blocks = keys.reshape(SEGMENT_TOTAL, BLOCK, KV_HEADS, HD)
    value_blocks = values.reshape(SEGMENT_TOTAL, BLOCK, KV_HEADS, HD)
    query_parts = queries.reshape(N_KV, per_dev, BLOCK, KV_HEADS, groups, HD)
    chosen_parts = chosen.reshape(N_KV, per_dev, NSEL)
    firsts = (jnp.arange(N_KV) * per_dev).astype(jnp.int32)
    limit = live_length[0]

    def attend(item):
        q_part, picks, first = item
        valid = picks >= 0
        safe = jnp.maximum(picks, 0)
        near_keys = key_blocks[safe].astype(jnp.float32)
        near_values = value_blocks[safe].astype(jnp.float32)
        scores = jnp.einsum("jqkgd,jnbkd->jkgqnb", q_part.astype(jnp.float32), near_keys) * (HD ** -0.5)
        query_pos = (first + jnp.arange(per_dev, dtype=jnp.int32))[:, None] * BLOCK + jnp.arange(BLOCK, dtype=jnp.int32)[None, :]
        key_pos = safe[:, :, None] * BLOCK + jnp.arange(BLOCK, dtype=jnp.int32)[None, None, :]
        allowed = valid[:, None, :, None] & (key_pos[:, None, :, :] <= query_pos[:, :, None, None])
        masked = jnp.where(allowed[:, None, None], scores, -jnp.inf)
        top = jnp.max(masked, axis=(4, 5), keepdims=True)
        weights = jnp.exp(masked - top)
        total = jnp.sum(weights, axis=(4, 5))
        rounded = lax.optimization_barrier(weights.astype(jnp.bfloat16)).astype(jnp.float32)
        summed = jnp.einsum("jkgqnb,jnbkd->jqkgd", rounded, near_values)
        result = summed / jnp.transpose(total, (0, 3, 1, 2))[..., None]
        live = query_pos < limit
        result = jnp.where(live[:, :, None, None, None], result, 0.0)
        return result.astype(jnp.bfloat16)

    attended = lax.map(attend, (query_parts, chosen_parts, firsts)).reshape(TOKENS, Q_WIDTH)
    return jnp.dot(attended, out_weight, preferred_element_type=jnp.float32).astype(jnp.bfloat16)
```

```python
import functools

import jax
import jax.numpy as jnp
from jax import lax
from jax.experimental import pallas as pl
from jax.experimental.pallas import tpu as pltpu
from jax.sharding import PartitionSpec as P

HD = 128
BLOCK = 32
CAP = 2
MESH = pl.DeviceIdType.MESH


def gathered_body(tokens, query_weight, key_weight, value_weight, out_weight, chosen, live_length):
    rows = tokens.shape[0]
    per_dev = rows // BLOCK
    owners = lax.axis_size("kv")
    me = lax.axis_index("kv")

    def add_rows(piece):
        return jnp.dot(tokens, piece, preferred_element_type=jnp.float32)

    queries = add_rows(lax.all_gather(query_weight, "kv", axis=0, tiled=True))
    keys = add_rows(lax.all_gather(key_weight, "kv", axis=0, tiled=True))
    values = add_rows(lax.all_gather(value_weight, "kv", axis=0, tiled=True))
    queries = queries.astype(jnp.bfloat16)
    paired = jnp.concatenate([keys.astype(jnp.bfloat16), values.astype(jnp.bfloat16)], axis=1)
    width = paired.shape[1]
    local_blocks = paired.reshape(per_dev, BLOCK, width)
    valid = chosen >= 0
    safe = jnp.maximum(chosen, 0)
    blocks_all = owners * per_dev
    hits = (safe[:, :, None] == jnp.arange(blocks_all, dtype=jnp.int32)[None, None, :]) & valid[
        :, :, None
    ]
    needed = jnp.any(hits, axis=(0, 1)).reshape(owners, per_dev)
    needed = needed & (jnp.arange(owners, dtype=jnp.int32) != me)[:, None]
    ranks = jnp.cumsum(needed.astype(jnp.int32), axis=1)
    local_ids = jnp.arange(per_dev, dtype=jnp.int32)
    slot_lists = []
    for slot in range(CAP):
        marked = needed & (ranks == slot + 1)
        found = jnp.any(marked, axis=1)
        where_at = jnp.sum(jnp.where(marked, local_ids[None, :], 0), axis=1)
        slot_lists.append(jnp.where(found, where_at, -1))
    wanted = jnp.stack(slot_lists, axis=1)
    requested = lax.all_to_all(wanted, "kv", split_axis=0, concat_axis=0, tiled=True)
    outgoing = local_blocks[jnp.maximum(requested, 0)]
    outgoing = jnp.where((requested >= 0)[:, :, None, None], outgoing, jnp.zeros((), jnp.bfloat16))
    incoming = lax.all_to_all(outgoing, "kv", split_axis=0, concat_axis=0, tiled=True)
    table = jnp.concatenate([incoming.reshape(owners * CAP, BLOCK, width), local_blocks], axis=0)
    segment_retainer = safe // per_dev
    local_of = safe % per_dev
    match = (wanted[None, None, :, :] == local_of[:, :, None, None]) & (
        jnp.arange(owners, dtype=jnp.int32)[None, None, :, None]
        == segment_retainer[:, :, None, None]
    )
    slot_index = jnp.arange(owners * CAP, dtype=jnp.int32).reshape(owners, CAP)
    remote_at = jnp.sum(jnp.where(match, slot_index[None, None], 0), axis=(2, 3))
    position = jnp.where(segment_retainer == me, owners * CAP + local_of, remote_at)
    picked = table[position]
    near_keys = picked[..., :HD]
    near_values = picked[..., HD:]
    grouped = queries.reshape(per_dev, BLOCK, -1, HD)
    scores = jnp.einsum(
        "jqhd,jnbd->jhqnb", grouped, near_keys, preferred_element_type=jnp.float32
    ) * HD ** (-0.5)
    query_pos = (me * per_dev + jnp.arange(per_dev, dtype=jnp.int32))[:, None] * BLOCK + jnp.arange(
        BLOCK, dtype=jnp.int32
    )[None, :]
    key_pos = safe[:, :, None] * BLOCK + jnp.arange(BLOCK, dtype=jnp.int32)[None, None, :]
    allowed = valid[:, None, :, None] & (key_pos[:, None, :, :] <= query_pos[:, :, None, None])
    masked = jnp.where(allowed[:, None], scores, -jnp.inf)
    top = jnp.max(masked, axis=(3, 4), keepdims=True)
    weights = jnp.exp(masked - top)
    total = jnp.sum(weights, axis=(3, 4))
    summed = jnp.einsum(
        "jhqnb,jnbd->jqhd",
        weights.astype(jnp.bfloat16),
        near_values,
        preferred_element_type=jnp.float32,
    )
    result = summed / jnp.transpose(total, (0, 2, 1))[..., None]
    live = query_pos < live_length[0]
    result = jnp.where(live[:, :, None, None], result, 0.0)
    attended = result.astype(jnp.bfloat16).reshape(rows, -1)
    every_head = lax.all_gather(attended, "tp", axis=1, tiled=True)
    mixed = jnp.dot(
        every_head,
        lax.all_gather(out_weight, "kv", axis=0, tiled=True),
        preferred_element_type=jnp.float32,
    )
    return mixed.astype(jnp.bfloat16)


HALF = 2
MODES = "qqqh"
ORDER = (
    ("own", 0), ("own", 1), ("own", 2), ("w", 0), ("t", 0), ("w", 1), ("t", 1), ("w", 2),
    ("own", 0, "o"), ("t", 2), ("w", 3), ("t", 3), ("w", 4), ("own", 1, "o"), ("w", 5), ("w", 6),
    ("own", 2, "o"), ("w", 7), ("o", 0, 0), ("kv1",), ("o", 0, 1), ("oc", 0, 0), ("w", 8),
    ("own", 3, "o"), ("kv2",), ("oc", 0, 1), ("o", 0, 2), ("q1", 0), ("q1", 1), ("oc", 0, 2),
    ("o", 1, 0), ("o", 1, 1), ("oc", 1, 0), ("q2", 0), ("o", 1, 2), ("oc", 1, 1), ("q2", 1),
    ("o", 2, 0), ("oc", 1, 2), ("o", 2, 1), ("att", 2, 0), ("oc", 2, 0), ("o", 2, 2),
    ("oc", 2, 1), ("att", 2, 1), ("share",), ("o", 3, 0), ("oc", 2, 2), ("o", 3, 1), ("o", 3, 2),
    ("fin", 0), ("fin", 1), ("fin", 2), ("oc", 3, 0), ("oc", 3, 1), ("oc", 3, 2), ("fin", 3),
)


def pick(at, values):
    out = jnp.int32(values[0])
    for i, v in enumerate(values[1:]):
        out = jnp.where(at == i + 1, jnp.int32(v), out)
    return out


class Mover:
    def __init__(self, sends, recvs):
        self.sends, self.recvs = sends, recvs
        self.begun = []

    def copy(self, src, dst, send, recv, target):
        return pltpu.make_async_remote_copy(
            src_ref=src, dst_ref=dst, send_sem=self.sends.at[send], recv_sem=self.recvs.at[recv],
            device_id=target, device_id_type=MESH,
        )

    def begin(self, c, when=None):
        if when is None:
            c.start()
        else:
            pl.when(when)(c.start)
        self.begun.append((c, when))

    def finish(self):
        for c, when in self.begun:
            if when is None:
                c.wait_send()
            else:
                pl.when(when)(c.wait_send)


def kernel(
    n, chosen, live, tokens, query_w, key_w, value_w, out_w, listing, mixed,
    tok, other, weights, outs, lists, table, picked, mine_kv, mine_q, away, back,
    queries, bias, attended, staged, local_sem, send_sem, recv_sem, out_sem,
):
    dp, me, tp = lax.axis_index("dp"), lax.axis_index("kv"), lax.axis_index("tp")
    x_at, y_at = lax.rem(dp, 2), lax.div(dp, 2)
    right, left = jnp.minimum(me + 1, n - 1), jnp.maximum(me - 1, 0)
    to_x = {"dp": 2 * y_at + (1 - x_at)}
    to_y = {"dp": 2 * (1 - y_at) + x_at}
    dp_x, dp_y = 2 * y_at + (1 - x_at), 2 * (1 - y_at) + x_at
    dp_far = 2 * (1 - y_at) + (1 - x_at)
    side = lax.rem(x_at + y_at, 2)
    partner = {"tp": 1 - tp}
    rows = other.shape[0]
    depth = tok.shape[1]
    per_dev = rows // BLOCK
    seg = depth // n
    half_seg = seg // 2
    width = weights.shape[1]
    groups = weights.shape[0] // depth
    owned = outs.shape[0] // len(MODES) // n
    tall = n * owned
    tile = outs.shape[1]
    is_end = jnp.logical_or(me == 0, me == n - 1)
    near = [pick(me, v) for v in ((1, 2, 1, 2), (2, 0, 3, 1), (3, 3, 0, 0))]
    mover = Mover(send_sem, recv_sem)

    loads = []

    def load(src, dst):
        c = pltpu.make_async_copy(src, dst, local_sem.at[len(loads)])
        c.start()
        loads.append(c)
        return c

    my_rows = pl.ds(pl.multiple_of(x_at * seg, seg), seg)

    def slab(group):
        return pl.ds(pl.multiple_of(group * depth + me * seg, seg), seg)

    kv_load = [
        load(key_w.at[my_rows, :], weights.at[slab(0), :HD]),
        load(value_w.at[my_rows, :], weights.at[slab(0), HD:]),
    ]
    q_load = [
        load(query_w.at[my_rows, i * width : (i + 1) * width], weights.at[slab(1 + i), :])
        for i in range(groups - 1)
    ]
    tok_load = [
        load(
            tokens.at[:, pl.ds(pl.multiple_of((2 * k + x_at) * seg, seg), seg)],
            tok.at[:, k * seg : (k + 1) * seg],
        )
        for k in range(n)
    ]
    o_load = [
        load(
            out_w.at[:, s * tile : (s + 1) * tile],
            outs.at[pl.ds(pl.multiple_of(s * tall + me * owned, owned), owned), :],
        )
        for s in range(len(MODES))
    ]
    list_load = load(listing, lists.at[me])

    barrier = pltpu.get_barrier_semaphore()
    greeted = [{"kv": lax.rem(me + step, n)} for step in range(1, n)] + [to_x, to_y, partner]
    for target in greeted:
        pl.semaphore_signal(barrier, inc=1, device_id=target, device_id_type=MESH)
    pl.semaphore_wait(barrier, len(greeted))

    W = 0
    O = W + groups * n * 3
    T = O + len(MODES) * n * 6
    L = T + 2 * n
    K = L + n
    Y = K + n
    S = Y + groups

    my_part = pl.ds(pl.multiple_of(tp * (rows // 2), rows // 2), rows // 2)
    their_part = pl.ds(pl.multiple_of((1 - tp) * (rows // 2), rows // 2), rows // 2)

    def t_copy(k):
        cols = pl.ds(pl.multiple_of((2 * k + 1 - x_at) * seg, seg), seg)
        return mover.copy(
            tokens.at[my_part, cols], other.at[my_part, k * seg : (k + 1) * seg], T + k, T + k, to_x
        )

    def t_share(k, part):
        piece = other.at[part, k * seg : (k + 1) * seg]
        return mover.copy(piece, piece, T + n + k, T + n + k, partner)

    for k in range(n):
        mover.begin(t_copy(k))

    def l_copy(step):
        return mover.copy(
            listing, lists.at[me], L + step, L + step, {"kv": jnp.maximum(me - step, 0)}
        )

    for step in range(1, n):
        mover.begin(l_copy(step), me >= step)

    def w_piece(group, owner, which):
        start = group * depth + owner * seg + which * half_seg
        return weights.at[pl.ds(pl.multiple_of(start, half_seg), half_seg), :]

    def w_copy(group, owner, which, kind, target, sent=None):
        at = W + (group * n + owner) * 3
        piece = w_piece(group, owner, which)
        return mover.copy(piece, piece, at + (kind if sent is None else sent), at + kind, target)

    def w_own(group):
        for c in (kv_load if group == 0 else q_load[group - 1 : group]):
            c.wait()
        mover.begin(w_copy(group, me, y_at, 0, {"kv": right}), me < n - 1)
        mover.begin(w_copy(group, me, y_at, 0, {"kv": left}, 2), me > 0)

    def w_step(p):
        inner = (p // 2, p % 2) if p < 2 * groups else (p - 2 * groups, 2)
        group = jnp.where(is_end, p % groups, inner[0])
        owner = jnp.where(is_end, near[p // groups], near[inner[1]])
        w_copy(group, owner, y_at, 0, {"kv": right}).wait_recv()
        mover.begin(
            w_copy(group, owner, y_at, 0, {"kv": right}), jnp.logical_and(owner < me, me < n - 1)
        )
        mover.begin(w_copy(group, owner, y_at, 0, {"kv": left}), jnp.logical_and(owner > me, me > 0))
        mover.begin(w_copy(group, owner, y_at, 1, to_y))

    def w_arrive(group):
        for owner in near:
            w_copy(group, owner, 1 - y_at, 1, to_y).wait_recv()

    def o_piece(s, owner, index, count):
        size = owned // count
        return outs.at[
            pl.ds(pl.multiple_of(s * tall + owner * owned + index * size, size), size), :
        ]

    def o_copy(s, owner, index, count, kind, target, sent=None):
        at = O + (s * n + owner) * 6
        piece = o_piece(s, owner, index, count)
        return mover.copy(piece, piece, at + (kind if sent is None else sent), at + kind, target)

    def o_carried(s, owner):
        return (s, owner, dp, 4) if MODES[s] == "q" else (s, owner, side, 2)

    def o_own(s):
        o_load[s].wait()
        mover.begin(o_copy(*o_carried(s, me), 0, {"kv": right}), me < n - 1)
        mover.begin(o_copy(*o_carried(s, me), 0, {"kv": left}, 5), me > 0)

    def o_step(s, slot):
        owner = near[slot]
        carried = o_carried(s, owner)
        o_copy(*carried, 0, {"kv": right}).wait_recv()
        mover.begin(o_copy(*carried, 0, {"kv": right}), jnp.logical_and(owner < me, me < n - 1))
        mover.begin(o_copy(*carried, 0, {"kv": left}), jnp.logical_and(owner > me, me > 0))
        if MODES[s] == "q":
            mover.begin(o_copy(*carried, 1, to_x))
            mover.begin(o_copy(*carried, 2, to_y))
        else:
            mover.begin(o_copy(s, owner, 2 * side, 4, 1, to_x))
            mover.begin(o_copy(s, owner, 2 * side + 1, 4, 2, to_y))

    def o_corner(s, slot):
        owner = near[slot]
        if MODES[s] == "q":
            o_copy(s, owner, dp_x, 4, 1, to_x).wait_recv()
            mover.begin(o_copy(s, owner, 2 * dp_x, 8, 4, to_y))
            o_copy(s, owner, dp_y, 4, 2, to_y).wait_recv()
            mover.begin(o_copy(s, owner, 2 * dp_y + 1, 8, 3, to_x))
        else:
            o_copy(s, owner, 2 * (1 - side), 4, 1, to_x).wait_recv()
            o_copy(s, owner, 2 * (1 - side) + 1, 4, 2, to_y).wait_recv()

    def o_arrive(s):
        if MODES[s] == "q":
            for owner in near:
                o_copy(s, owner, 2 * dp_far, 8, 4, to_y).wait_recv()
                o_copy(s, owner, 2 * dp_far + 1, 8, 3, to_x).wait_recv()

    def part(source, group):
        return jnp.dot(
            source[...], weights[group * depth : (group + 1) * depth, :],
            preferred_element_type=jnp.float32,
        )

    def y_copy(group):
        return mover.copy(away.at[group], back.at[group], Y + group, Y + group, to_x)

    def project(group):
        w_arrive(group)
        away[group] = part(other, group).astype(jnp.bfloat16)
        mover.begin(y_copy(group))
        if group == 0:
            mine_kv[...] = part(tok, group)
        else:
            mine_q[:, (group - 1) * width : group * width] = part(tok, group)

    slots = CAP * BLOCK
    local_at = n * slots

    def found(listed, block):
        return jnp.max((listed == block).astype(jnp.float32), axis=(0, 1), keepdims=True)

    def marks(listed, first):
        rank = jnp.zeros((1, 1), jnp.float32)
        out = [[] for _ in range(CAP)]
        for b in range(per_dev):
            one = found(listed, first + b)
            rank = rank + one
            for s in range(CAP):
                out[s].append(jnp.where(rank == s + 1, one, 0.0))
        return out

    def k_copy(step):
        return mover.copy(
            picked.at[step - 1], table.at[pl.ds(pl.multiple_of(me * slots, slots), slots), :],
            K + step, K + step, {"kv": jnp.minimum(me + step, n - 1)},
        )

    def k_arrive():
        for step in range(1, n):
            owner = jnp.maximum(me - step, 0)
            c = mover.copy(
                picked.at[step - 1],
                table.at[pl.ds(pl.multiple_of(owner * slots, slots), slots), :],
                K + step, K + step, {"kv": jnp.minimum(me + step, n - 1)},
            )
            pl.when(me >= step)(c.wait_recv)

    def share_blocks():
        y_copy(0).wait_recv()
        full = (mine_kv[...] + back[0].astype(jnp.float32)).astype(jnp.bfloat16)
        table[local_at : local_at + rows, :] = full
        full = full.astype(jnp.float32)
        for step in range(1, n):
            pl.when(me + step < n)(l_copy(step).wait_recv)
        for step in range(1, n):

            def send_to(step=step):
                which = marks(lists[me + step], me * per_dev)
                for s in range(CAP):
                    kept = jnp.zeros((BLOCK, full.shape[1]), jnp.float32)
                    for b in range(per_dev):
                        kept = kept + which[s][b] * full[b * BLOCK : (b + 1) * BLOCK, :]
                    picked[step - 1, s * BLOCK : (s + 1) * BLOCK, :] = kept.astype(jnp.bfloat16)

            pl.when(me + step < n)(send_to)
            mover.begin(k_copy(step), me + step < n)

    def build_bias():
        list_load.wait()
        listed = lists[me]
        seq = bias.shape[1]
        column = lax.broadcasted_iota(jnp.int32, (8, seq), 1)
        block = me * per_dev + lax.div(column - local_at, BLOCK)
        for owner in range(n):
            which = marks(listed, owner * per_dev)
            for s in range(CAP):
                ident = jnp.full((1, 1), -2.0, jnp.float32)
                for b in range(per_dev):
                    ident = jnp.where(which[s][b] > 0.5, float(owner * per_dev + b), ident)
                ident = jnp.where(me == owner, -2.0, ident).astype(jnp.int32)
                block = jnp.where(lax.div(column, BLOCK) == owner * CAP + s, ident, block)
        at = block * BLOCK + lax.rem(column, BLOCK)
        at = jnp.concatenate([at] * (BLOCK // 8), axis=0)
        row = lax.broadcasted_iota(jnp.int32, (BLOCK, seq), 0)
        for j in range(per_dev):
            open_to = jnp.full((8, seq), -jnp.inf, jnp.float32)
            for e in range(chosen.shape[1]):
                open_to = jnp.where(block == chosen[j, e], 0.0, open_to)
            spread = jnp.concatenate([open_to] * (BLOCK // 8), axis=0)
            causal = at <= row + (me * rows + j * BLOCK)
            bias[j * BLOCK : (j + 1) * BLOCK, :] = jnp.where(causal, spread, -jnp.inf)

    def queries_done(half):
        y_copy(1 + half).wait_recv()
        cols = slice(half * width, (half + 1) * width)
        queries[:, cols] = (
            mine_q[:, cols] + back[1 + half].astype(jnp.float32)
        ).astype(jnp.bfloat16)

    def attend(count, index):
        if index == 0:
            k_arrive()
        alive = me * rows + lax.broadcasted_iota(jnp.int32, (rows, HD), 0) < live[0]
        for h in range(count * index, count * (index + 1)):
            cols = slice(h * HD, (h + 1) * HD)
            scores = lax.dot_general(
                queries[:, cols], table[:, :HD], (((1,), (1,)), ((), ())),
                preferred_element_type=jnp.float32,
            )
            masked = scores * HD ** (-0.5) + bias[...]
            top = jnp.max(masked, axis=1, keepdims=True)
            probs = jnp.exp(masked - top)
            total = jnp.sum(probs, axis=1, keepdims=True)
            summed = jnp.dot(
                probs.astype(jnp.bfloat16), table[:, HD:], preferred_element_type=jnp.float32
            )
            attended[tp, :, cols] = jnp.where(alive, summed / total, 0.0).astype(jnp.bfloat16)

    def share_copy(at):
        return mover.copy(attended.at[at], attended.at[at], S, S, partner)

    wide = queries.shape[1]
    stores = []
    shared = []

    def final(s):
        if not shared:
            share_copy(1 - tp).wait_recv()
            shared.append(True)
        o_arrive(s)
        acc = jnp.dot(
            attended[0], outs[s * tall : s * tall + wide, :], preferred_element_type=jnp.float32
        )
        acc += jnp.dot(
            attended[1], outs[s * tall + wide : (s + 1) * tall, :],
            preferred_element_type=jnp.float32,
        )
        staged[s] = acc.astype(jnp.bfloat16)
        c = pltpu.make_async_copy(
            staged.at[s], mixed.at[:, s * tile : (s + 1) * tile], out_sem.at[s]
        )
        c.start()
        stores.append(c)

    shared_out = []
    built = []
    for step in ORDER:
        name, args = step[0], step[1:]
        if name == "own":
            o_own(args[0]) if len(args) > 1 else w_own(args[0])
        elif name == "w":
            if not built:
                for owner in range(n):
                    def clear(owner=owner):
                        table[owner * slots : (owner + 1) * slots, :] = jnp.zeros(
                            (slots, table.shape[1]), table.dtype
                        )
                    pl.when(owner >= me)(clear)
                build_bias()
                for c in tok_load:
                    c.wait()
                built.append(True)
            w_step(args[0])
        elif name == "t":
            t_copy(args[0]).wait_recv()
            mover.begin(t_share(args[0], my_part))
        elif name == "o":
            o_step(*args)
        elif name == "oc":
            o_corner(*args)
        elif name == "kv1":
            for k in range(n):
                t_share(k, their_part).wait_recv()
            project(0)
        elif name == "q1":
            project(1 + args[0])
        elif name == "kv2":
            share_blocks()
        elif name == "q2":
            queries_done(args[0])
        elif name == "att":
            attend(*args)
        elif name == "share":
            c = share_copy(tp)
            mover.begin(c)
        else:
            final(args[0])
    mover.finish()
    for c in stores:
        c.wait()


def woven_body(tokens, query_weight, key_weight, value_weight, out_weight, chosen, live_length):
    n = lax.axis_size("kv")
    rows, model = tokens.shape
    wide = query_weight.shape[1]
    depth = model // HALF
    width = 2 * HD
    groups = 1 + wide // width
    chunks = len(MODES)
    tile = out_weight.shape[1] // chunks
    slots = CAP * BLOCK
    total = n * slots + rows
    dma = pltpu.SemaphoreType.DMA
    bf16 = jnp.bfloat16
    f32 = jnp.float32
    anywhere = pl.BlockSpec(memory_space=pl.ANY)
    small = pl.BlockSpec(memory_space=pltpu.SMEM)
    sems = groups * n * 3 + chunks * n * 6 + 2 * n + n + n + groups + 1
    return pl.pallas_call(
        functools.partial(kernel, n),
        out_shape=jax.ShapeDtypeStruct((rows, out_weight.shape[1]), bf16),
        in_specs=[small, small] + [anywhere] * 6,
        out_specs=anywhere,
        scratch_shapes=[
            pltpu.VMEM((rows, depth), bf16),
            pltpu.VMEM((rows, depth), bf16),
            pltpu.VMEM((groups * depth, width), bf16),
            pltpu.VMEM((chunks * n * out_weight.shape[0], tile), bf16),
            pltpu.VMEM((n,) + chosen.shape, jnp.int32),
            pltpu.VMEM((total, width), bf16),
            pltpu.VMEM((n - 1, slots, width), bf16),
            pltpu.VMEM((rows, width), f32),
            pltpu.VMEM((rows, wide), f32),
            pltpu.VMEM((groups, rows, width), bf16),
            pltpu.VMEM((groups, rows, width), bf16),
            pltpu.VMEM((rows, wide), bf16),
            pltpu.VMEM((rows, total), f32),
            pltpu.VMEM((2, rows, wide), bf16),
            pltpu.VMEM((chunks, rows, tile), bf16),
            dma((2 + groups - 1 + n + chunks + 1,)),
            dma((sems,)),
            dma((sems,)),
            dma((chunks,)),
        ],
        compiler_params=pltpu.CompilerParams(
            collective_id=0, has_side_effects=True, vmem_limit_bytes=48 * 2**20
        ),
    )(chosen, live_length, tokens, query_weight, key_weight, value_weight, out_weight, chosen)


def solution(mesh):
    in_specs = (
        P(("dp", "kv"), None),
        P("kv", "tp"),
        P("kv", "tp"),
        P("kv", "tp"),
        P("kv", "tp"),
        P(("dp", "kv"), None),
        P("dp"),
    )
    out_specs = P(("dp", "kv"), "tp")
    fits = (mesh.shape["dp"], mesh.shape["kv"], mesh.shape["tp"]) == (4, 4, 2)
    body = woven_body if fits else gathered_body
    return jax.shard_map(body, mesh=mesh, in_specs=in_specs, out_specs=out_specs, check_vma=False)
```

```python
import functools
import math

import jax
import jax.numpy as jnp
from jax import lax
from jax.experimental import pallas as pl
from jax.experimental.pallas import tpu as pltpu
from jax.sharding import PartitionSpec as P

HD = 128
BLOCK = 32
CAP = 2
MESH = pl.DeviceIdType.MESH


def gathered_body(tokens, query_weight, key_weight, value_weight, out_weight, chosen, live_length):
    rows = tokens.shape[0]
    per_dev = rows // BLOCK
    owners = lax.axis_size("kv")
    me = lax.axis_index("kv")

    def add_rows(piece):
        return jnp.dot(tokens, piece, preferred_element_type=jnp.float32)

    queries = add_rows(lax.all_gather(query_weight, "kv", axis=0, tiled=True))
    keys = add_rows(lax.all_gather(key_weight, "kv", axis=0, tiled=True))
    values = add_rows(lax.all_gather(value_weight, "kv", axis=0, tiled=True))
    queries = queries.astype(jnp.bfloat16)
    paired = jnp.concatenate([keys.astype(jnp.bfloat16), values.astype(jnp.bfloat16)], axis=1)
    width = paired.shape[1]
    local_blocks = paired.reshape(per_dev, BLOCK, width)
    valid = chosen >= 0
    safe = jnp.maximum(chosen, 0)
    blocks_all = owners * per_dev
    hits = (safe[:, :, None] == jnp.arange(blocks_all, dtype=jnp.int32)[None, None, :]) & valid[
        :, :, None
    ]
    needed = jnp.any(hits, axis=(0, 1)).reshape(owners, per_dev)
    needed = needed & (jnp.arange(owners, dtype=jnp.int32) != me)[:, None]
    ranks = jnp.cumsum(needed.astype(jnp.int32), axis=1)
    local_ids = jnp.arange(per_dev, dtype=jnp.int32)
    slot_lists = []
    for slot in range(CAP):
        marked = needed & (ranks == slot + 1)
        found = jnp.any(marked, axis=1)
        where_at = jnp.sum(jnp.where(marked, local_ids[None, :], 0), axis=1)
        slot_lists.append(jnp.where(found, where_at, -1))
    wanted = jnp.stack(slot_lists, axis=1)
    requested = lax.all_to_all(wanted, "kv", split_axis=0, concat_axis=0, tiled=True)
    outgoing = local_blocks[jnp.maximum(requested, 0)]
    outgoing = jnp.where((requested >= 0)[:, :, None, None], outgoing, jnp.zeros((), jnp.bfloat16))
    incoming = lax.all_to_all(outgoing, "kv", split_axis=0, concat_axis=0, tiled=True)
    table = jnp.concatenate([incoming.reshape(owners * CAP, BLOCK, width), local_blocks], axis=0)
    segment_retainer = safe // per_dev
    local_of = safe % per_dev
    match = (wanted[None, None, :, :] == local_of[:, :, None, None]) & (
        jnp.arange(owners, dtype=jnp.int32)[None, None, :, None]
        == segment_retainer[:, :, None, None]
    )
    slot_index = jnp.arange(owners * CAP, dtype=jnp.int32).reshape(owners, CAP)
    remote_at = jnp.sum(jnp.where(match, slot_index[None, None], 0), axis=(2, 3))
    position = jnp.where(segment_retainer == me, owners * CAP + local_of, remote_at)
    picked = table[position]
    near_keys = picked[..., :HD]
    near_values = picked[..., HD:]
    grouped = queries.reshape(per_dev, BLOCK, -1, HD)
    scores = jnp.einsum(
        "jqhd,jnbd->jhqnb", grouped, near_keys, preferred_element_type=jnp.float32
    ) * HD ** (-0.5)
    query_pos = (me * per_dev + jnp.arange(per_dev, dtype=jnp.int32))[:, None] * BLOCK + jnp.arange(
        BLOCK, dtype=jnp.int32
    )[None, :]
    key_pos = safe[:, :, None] * BLOCK + jnp.arange(BLOCK, dtype=jnp.int32)[None, None, :]
    allowed = valid[:, None, :, None] & (key_pos[:, None, :, :] <= query_pos[:, :, None, None])
    masked = jnp.where(allowed[:, None], scores, -jnp.inf)
    top = jnp.max(masked, axis=(3, 4), keepdims=True)
    weights = jnp.exp(masked - top)
    total = jnp.sum(weights, axis=(3, 4))
    summed = jnp.einsum(
        "jhqnb,jnbd->jqhd",
        weights.astype(jnp.bfloat16),
        near_values,
        preferred_element_type=jnp.float32,
    )
    result = summed / jnp.transpose(total, (0, 2, 1))[..., None]
    live = query_pos < live_length[0]
    result = jnp.where(live[:, :, None, None], result, 0.0)
    attended = result.astype(jnp.bfloat16).reshape(rows, -1)
    every_head = lax.all_gather(attended, "tp", axis=1, tiled=True)
    mixed = jnp.dot(
        every_head,
        lax.all_gather(out_weight, "kv", axis=0, tiled=True),
        preferred_element_type=jnp.float32,
    )
    return mixed.astype(jnp.bfloat16)


HALF = 2
LEAST = 16
CUTS = {"q": 32, "p": 16}
MODES = "ppph"
WEIGHTS, OUTS, REST = range(3)
BULK = 3
ORDER_END = (
    ("owno", 1, 0), ("own", 0, 0), ("owno", 0, 0), ("owno", 2, 0), ("own", 1, 0), ("o", 0, 0),
    ("own", 2, 0), ("o", 1, 0), ("o", 2, 0), ("o", 0, 1), ("w", 0, 0), ("o", 2, 1), ("o", 1, 1),
    ("w", 1, 0), ("o", 1, 2), ("ocy", 0, 0), ("ocy", 2, 0), ("ocy", 1, 0), ("w", 0, 2),
    ("ocy", 1, 2), ("ocy", 1, 1), ("ocy", 0, 1), ("owno", 3, 0), ("w", 1, 1), ("t", 0, 0),
    ("w", 1, 2), ("ocy", 2, 1), ("w", 0, 1), ("o", 0, 2), ("q1", 0, 0), ("w", 2, 0),
    ("kv1", 0, 0), ("w", 2, 1), ("w", 2, 2), ("o", 2, 2), ("ocy", 0, 2), ("ocx", 2, 0),
    ("kv2", 0, 0), ("o", 3, 2), ("q1", 1, 0), ("ocy", 2, 2), ("ocx", 2, 1), ("o", 3, 0),
    ("ocx", 0, 1), ("q2", 0, 0), ("ocx", 2, 2), ("ocx", 1, 2), ("ocx", 0, 2), ("ocx", 0, 0),
    ("att", 0, 0), ("ocx", 1, 0), ("ocx", 1, 1), ("o", 3, 1), ("q2", 1, 0), ("att", 1, 0),
    ("share", 0, 0), ("fin", 2, 0), ("fin", 1, 0), ("fin", 0, 0), ("fin", 3, 0),
)
ORDER_INNER = (
    ("owno", 0, 0), ("owno", 1, 0), ("owno", 2, 0), ("o", 0, 0), ("own", 0, 0), ("o", 1, 0),
    ("w", 0, 1), ("ocy", 0, 0), ("o", 2, 0), ("ocy", 1, 0), ("o", 1, 1), ("own", 1, 0),
    ("t", 0, 0), ("o", 0, 1), ("w", 1, 1), ("o", 1, 2), ("w", 0, 2), ("w", 1, 0), ("w", 2, 1),
    ("w", 1, 2), ("w", 0, 0), ("o", 0, 2), ("own", 2, 0), ("ocy", 1, 1), ("ocy", 2, 0),
    ("w", 2, 0), ("w", 2, 2), ("o", 2, 1), ("ocy", 1, 2), ("ocx", 0, 0), ("ocx", 0, 1),
    ("ocy", 0, 1), ("ocx", 2, 0), ("o", 3, 1), ("q1", 0, 0), ("o", 2, 2), ("ocx", 1, 2),
    ("ocx", 1, 0), ("kv1", 0, 0), ("ocx", 1, 1), ("o", 3, 2), ("owno", 3, 0), ("q1", 1, 0),
    ("ocx", 0, 2), ("ocy", 0, 2), ("kv2", 0, 0), ("o", 3, 0), ("q2", 0, 0), ("ocy", 2, 1),
    ("att", 0, 0), ("q2", 1, 0), ("att", 1, 0), ("ocx", 2, 1), ("share", 0, 0), ("ocx", 2, 2),
    ("ocy", 2, 2), ("fin", 1, 0), ("fin", 3, 0), ("fin", 0, 0), ("fin", 2, 0),
)


def pick(at, values):
    out = jnp.int32(values[0])
    for i, v in enumerate(values[1:]):
        out = jnp.where(at == i + 1, jnp.int32(v), out)
    return out


class Run:
    def __init__(self, ends):
        self.ends = ends
        self.sent = [0] * BULK

    def begin(self, c, kind, ref):
        c.start()
        self.sent[kind] += math.prod(ref.shape)


def kernel(
    n, chosen, live, tokens, query_w, key_w, value_w, out_w, listing, mixed,
    tok, other, weights, outs, lists, table, picked, mine_kv, mine_q, away, back,
    queries, bias, attended, local_sem, send_sem, recv_sem,
):
    dp, me, tp = lax.axis_index("dp"), lax.axis_index("kv"), lax.axis_index("tp")
    x_at, y_at = lax.rem(dp, 2), lax.div(dp, 2)
    right, left = jnp.minimum(me + 1, n - 1), jnp.maximum(me - 1, 0)
    to_x = {"dp": 2 * y_at + (1 - x_at)}
    to_y = {"dp": 2 * (1 - y_at) + x_at}
    dp_x, dp_y = 2 * y_at + (1 - x_at), 2 * (1 - y_at) + x_at
    dp_far = 2 * (1 - y_at) + (1 - x_at)
    side = lax.rem(x_at + y_at, 2)
    partner = {"tp": 1 - tp}
    rows = other.shape[0]
    depth = tok.shape[1]
    per_dev = rows // BLOCK
    seg = depth // n
    half_seg = seg // 2
    width = weights.shape[1]
    groups = weights.shape[0] // depth
    chunks = len(MODES)
    owned = outs.shape[0] // chunks // n
    tall = n * owned
    tile = outs.shape[1]
    is_end = jnp.logical_or(me == 0, me == n - 1)
    inward = {"kv": jnp.where(me == 0, right, left)}
    near = [pick(me, v) for v in ((1, 2, 1, 2), (2, 0, 3, 1), (3, 3, 0, 0))]

    def load(src, dst, at):
        c = pltpu.make_async_copy(src, dst, local_sem.at[at])
        c.start()

    def loaded(ref, at):
        pltpu.make_async_copy(ref, ref, local_sem.at[at]).wait()

    def remote(src, dst, send, recv, target):
        return pltpu.make_async_remote_copy(
            src_ref=src, dst_ref=dst, send_sem=send_sem.at[send], recv_sem=recv_sem.at[recv],
            device_id=target, device_id_type=MESH,
        )

    def arrived(ref, recv):
        remote(ref, ref, 0, recv, partner).wait_recv()

    my_rows = pl.ds(pl.multiple_of(x_at * seg, seg), seg)

    def slab(group):
        return pl.ds(pl.multiple_of(group * depth + me * seg, seg), seg)

    load(key_w.at[my_rows, :], weights.at[slab(0), :HD], 0)
    load(value_w.at[my_rows, :], weights.at[slab(0), HD:], 0)
    for i in range(groups - 1):
        load(query_w.at[my_rows, i * width : (i + 1) * width], weights.at[slab(1 + i), :], 0)
    for s in range(chunks):
        load(
            out_w.at[:, s * tile : (s + 1) * tile],
            outs.at[pl.ds(pl.multiple_of(s * tall + me * owned, owned), owned), :],
            1,
        )
    for k in range(n):
        load(
            tokens.at[:, pl.ds(pl.multiple_of((2 * k + x_at) * seg, seg), seg)],
            tok.at[:, k * seg : (k + 1) * seg],
            2,
        )
    load(listing, lists.at[me], 3)

    with jax.named_scope("barrier"):
        barrier = pltpu.get_barrier_semaphore()
        greeted = [{"kv": lax.rem(me + step, n)} for step in range(1, n)] + [to_x, to_y, partner]
        for target in greeted:
            pl.semaphore_signal(barrier, inc=1, device_id=target, device_id_type=MESH)
        pl.semaphore_wait(barrier, len(greeted))

    others = n - 1
    W = 0
    WY = W + groups * others
    O = WY + groups
    OX = O + chunks * others
    OY = OX + chunks * others
    OC = OY + chunks * others
    T = OC + chunks
    L = T + 2
    K = L + others
    Y = K + others
    S = Y + groups

    def from_owner(owner, receiver):
        return lax.rem(owner + n - receiver, n) - 1

    my_part = pl.ds(pl.multiple_of(tp * (rows // 2), rows // 2), rows // 2)
    their_part = pl.ds(pl.multiple_of((1 - tp) * (rows // 2), rows // 2), rows // 2)
    for k in range(n):
        cols = pl.ds(pl.multiple_of((2 * k + 1 - x_at) * seg, seg), seg)
        remote(
            tokens.at[my_part, cols], other.at[my_part, k * seg : (k + 1) * seg], BULK + 2 * others, T, to_x
        ).start()

    def t_share(run):
        piece = other.at[my_part, :]
        arrived(piece, T)
        run.begin(remote(piece, piece, REST, T + 1, partner), REST, piece)

    def l_copy(step):
        return remote(
            listing, lists.at[me], BULK + step - 1, L + step - 1, {"kv": jnp.maximum(me - step, 0)}
        )

    for step in range(1, n):
        pl.when(me >= step)(l_copy(step).start)

    def z_targets(run):
        return [inward] if run.ends else [{"kv": right}, {"kv": left}]

    def w_piece(group, owner, which):
        start = group * depth + owner * seg + which * half_seg
        return weights.at[pl.ds(pl.multiple_of(start, half_seg), half_seg), :]

    def w_own(run, group):
        piece = w_piece(group, me, y_at)
        for target in z_targets(run):
            recv = W + group * others + from_owner(me, target["kv"])
            run.begin(remote(piece, piece, WEIGHTS, recv, target), WEIGHTS, piece)

    def w_step(run, group, slot):
        owner = near[slot]
        piece = w_piece(group, owner, y_at)
        arrived(piece, W + group * others + from_owner(owner, me))
        if not run.ends:
            to = jnp.where(owner < me, right, left)
            recv = W + group * others + from_owner(owner, to)
            run.begin(remote(piece, piece, WEIGHTS, recv, {"kv": to}), WEIGHTS, piece)
        run.begin(remote(piece, piece, WEIGHTS, WY + group, to_y), WEIGHTS, piece)

    def w_arrive(group):
        arrived(weights.at[: others * half_seg, :], WY + group)

    quarter = owned // 4

    def o_piece(s, owner, first, size):
        start = s * tall + owner * owned + first
        return outs.at[pl.ds(pl.multiple_of(start, LEAST), size), :]

    def o_send(run, piece, recv, target):
        run.begin(remote(piece, piece, OUTS, recv, target), OUTS, piece)

    def carried(s, owner):
        if MODES[s] in CUTS:
            return o_piece(s, owner, dp * quarter, quarter)
        return o_piece(s, owner, side * 2 * quarter, 2 * quarter)

    def o_own(run, s):
        for target in z_targets(run):
            o_send(run, carried(s, me), O + s * others + from_owner(me, target["kv"]), target)

    def o_step(run, s, slot):
        owner = near[slot]
        piece = carried(s, owner)
        arrived(piece, O + s * others + from_owner(owner, me))
        if not run.ends:
            to = jnp.where(owner < me, right, left)
            o_send(run, piece, O + s * others + from_owner(owner, to), {"kv": to})
        if MODES[s] in CUTS:
            at = s * others + from_owner(owner, me)
            o_send(run, piece, OX + at, to_x)
            o_send(run, piece, OY + at, to_y)
        else:
            o_send(run, o_piece(s, owner, 2 * side * quarter, quarter), OC + s, to_x)
            o_send(run, o_piece(s, owner, (2 * side + 1) * quarter, quarter), OC + s, to_y)

    def o_turn(run, s, slot, along_x):
        owner, cut = near[slot], CUTS[MODES[s]]
        at = s * others + from_owner(owner, me)
        if along_x:
            arrived(o_piece(s, owner, dp_x * quarter, quarter), OX + at)
            o_send(run, o_piece(s, owner, dp_x * quarter, cut), OC + s, to_y)
        else:
            arrived(o_piece(s, owner, dp_y * quarter, quarter), OY + at)
            o_send(run, o_piece(s, owner, dp_y * quarter + cut, quarter - cut), OC + s, to_x)

    def o_arrive(s):
        count = 1 if MODES[s] in CUTS else 2
        arrived(outs.at[: others * count * quarter, :], OC + s)

    def part(source, group):
        return jnp.dot(
            source[...], weights[group * depth : (group + 1) * depth, :],
            preferred_element_type=jnp.float32,
        )

    def y_copy(group):
        return remote(away.at[group], back.at[group], REST, Y + group, to_x)

    def project(run, group):
        w_arrive(group)
        away[group] = part(other, group).astype(jnp.bfloat16)
        run.begin(y_copy(group), REST, away.at[group])
        if group == 0:
            mine_kv[...] = part(tok, group)
        else:
            mine_q[:, (group - 1) * width : group * width] = part(tok, group)

    slots = CAP * BLOCK
    local_at = n * slots

    def found(listed, block):
        return jnp.max((listed == block).astype(jnp.float32), axis=(0, 1), keepdims=True)

    def marks(listed, first):
        rank = jnp.zeros((1, 1), jnp.float32)
        out = [[] for _ in range(CAP)]
        for b in range(per_dev):
            one = found(listed, first + b)
            rank = rank + one
            for s in range(CAP):
                out[s].append(jnp.where(rank == s + 1, one, 0.0))
        return out

    def k_copy(step):
        return remote(
            picked.at[step - 1], table.at[pl.ds(pl.multiple_of(me * slots, slots), slots), :],
            BULK + others + step - 1, K + step - 1, {"kv": jnp.minimum(me + step, n - 1)},
        )

    def k_arrive():
        for step in range(1, n):
            pl.when(me >= step)(k_copy(step).wait_recv)

    def share_blocks(run):
        y_copy(0).wait_recv()
        full = (mine_kv[...] + back[0].astype(jnp.float32)).astype(jnp.bfloat16)
        table[local_at : local_at + rows, :] = full
        full = full.astype(jnp.float32)
        for step in range(1, n):
            pl.when(me + step < n)(l_copy(step).wait_recv)
        for step in range(1, n):

            def send_to(step=step):
                which = marks(lists[me + step], me * per_dev)
                for s in range(CAP):
                    kept = jnp.zeros((BLOCK, full.shape[1]), jnp.float32)
                    for b in range(per_dev):
                        kept = kept + which[s][b] * full[b * BLOCK : (b + 1) * BLOCK, :]
                    picked[step - 1, s * BLOCK : (s + 1) * BLOCK, :] = kept.astype(jnp.bfloat16)

            pl.when(me + step < n)(send_to)
            pl.when(me + step < n)(k_copy(step).start)

    def build_bias():
        loaded(lists.at[me], 3)
        listed = lists[me]
        seq = bias.shape[1]
        column = lax.broadcasted_iota(jnp.int32, (8, seq), 1)
        block = me * per_dev + lax.div(column - local_at, BLOCK)
        for owner in range(n):
            which = marks(listed, owner * per_dev)
            for s in range(CAP):
                ident = jnp.full((1, 1), -2.0, jnp.float32)
                for b in range(per_dev):
                    ident = jnp.where(which[s][b] > 0.5, float(owner * per_dev + b), ident)
                ident = jnp.where(me == owner, -2.0, ident).astype(jnp.int32)
                block = jnp.where(lax.div(column, BLOCK) == owner * CAP + s, ident, block)
        at = block * BLOCK + lax.rem(column, BLOCK)
        at = jnp.concatenate([at] * (BLOCK // 8), axis=0)
        row = lax.broadcasted_iota(jnp.int32, (BLOCK, seq), 0)
        for j in range(per_dev):
            open_to = jnp.full((8, seq), -jnp.inf, jnp.float32)
            for e in range(chosen.shape[1]):
                open_to = jnp.where(block == chosen[j, e], 0.0, open_to)
            spread = jnp.concatenate([open_to] * (BLOCK // 8), axis=0)
            causal = at <= row + (me * rows + j * BLOCK)
            bias[j * BLOCK : (j + 1) * BLOCK, :] = jnp.where(causal, spread, -jnp.inf)

    def queries_done(half):
        y_copy(1 + half).wait_recv()
        cols = slice(half * width, (half + 1) * width)
        queries[:, cols] = (
            mine_q[:, cols] + back[1 + half].astype(jnp.float32)
        ).astype(jnp.bfloat16)

    def attend(count, index):
        if index == 0:
            k_arrive()
        alive = me * rows + lax.broadcasted_iota(jnp.int32, (rows, HD), 0) < live[0]
        for h in range(count * index, count * (index + 1)):
            cols = slice(h * HD, (h + 1) * HD)
            scores = lax.dot_general(
                queries[:, cols], table[:, :HD], (((1,), (1,)), ((), ())),
                preferred_element_type=jnp.float32,
            )
            masked = scores * HD ** (-0.5) + bias[...]
            top = jnp.max(masked, axis=1, keepdims=True)
            probs = jnp.exp(masked - top)
            total = jnp.sum(probs, axis=1, keepdims=True)
            summed = jnp.dot(
                probs.astype(jnp.bfloat16), table[:, HD:], preferred_element_type=jnp.float32
            )
            attended[tp, :, cols] = jnp.where(alive, summed / total, 0.0).astype(jnp.bfloat16)

    def share(run):
        piece = attended.at[tp]
        run.begin(remote(piece, piece, REST, S, partner), REST, piece)
        arrived(attended.at[1 - tp], S)

    wide = queries.shape[1]

    def final(s):
        o_arrive(s)
        acc = jnp.dot(
            attended[0], outs[s * tall : s * tall + wide, :], preferred_element_type=jnp.float32
        )
        acc += jnp.dot(
            attended[1], outs[s * tall + wide : (s + 1) * tall, :],
            preferred_element_type=jnp.float32,
        )
        mixed[:, s * tile : (s + 1) * tile] = acc.astype(jnp.bfloat16)

    def settle():
        for owner in range(n):

            def clear(owner=owner):
                table[owner * slots : (owner + 1) * slots, :] = jnp.zeros(
                    (slots, table.shape[1]), table.dtype
                )

            pl.when(owner >= me)(clear)
        build_bias()
        loaded(tok, 2)

    def act(run, name, i, j):
        if name == "own":
            w_own(run, i)
        elif name == "owno":
            o_own(run, i)
        elif name == "t":
            t_share(run)
        elif name == "w":
            w_step(run, i, j)
        elif name == "o":
            o_step(run, i, j)
        elif name == "ocx" or name == "ocy":
            o_turn(run, i, j, name == "ocx")
        elif name == "kv1":
            project(run, 0)
        elif name == "kv2":
            share_blocks(run)
        elif name == "q1":
            project(run, 1 + i)
        elif name == "q2":
            queries_done(i)
        elif name == "att":
            attend(width // HD, i)
        elif name == "share":
            share(run)
        else:
            final(i)

    def follow(order, ends):
        run = Run(ends)
        begun = False
        projected = False
        for name, i, j in order:
            if not begun and not name.startswith("own"):
                settle()
                begun = True
            if not projected and name in ("kv1", "q1"):
                arrived(other.at[their_part, :], T + 1)
                projected = True
            with jax.named_scope(f"{name}_{i}_{j}"):
                act(run, name, i, j)
        with jax.named_scope("sent"):
            for kind, size in enumerate(run.sent):
                ref = outs.at[: size // tile, :]
                remote(ref, ref, kind, 0, partner).wait_send()

    loaded(weights.at[: groups * seg, :], 0)
    loaded(outs.at[: chunks * owned, :], 1)
    pl.when(is_end)(functools.partial(follow, ORDER_END, True))
    pl.when(jnp.logical_not(is_end))(functools.partial(follow, ORDER_INNER, False))
    ref = other.at[my_part, :]
    remote(ref, ref, BULK + 2 * others, T, to_x).wait_send()
    for step in range(1, n):
        pl.when(me >= step)(l_copy(step).wait_send)
        pl.when(me + step < n)(k_copy(step).wait_send)


def woven_body(tokens, query_weight, key_weight, value_weight, out_weight, chosen, live_length):
    n = lax.axis_size("kv")
    rows, model = tokens.shape
    wide = query_weight.shape[1]
    depth = model // HALF
    width = 2 * HD
    groups = 1 + wide // width
    chunks = len(MODES)
    tile = out_weight.shape[1] // chunks
    slots = CAP * BLOCK
    total = n * slots + rows
    dma = pltpu.SemaphoreType.DMA
    bf16 = jnp.bfloat16
    f32 = jnp.float32
    anywhere = pl.BlockSpec(memory_space=pl.ANY)
    small = pl.BlockSpec(memory_space=pltpu.SMEM)
    others = n - 1
    arrivals = groups * (others + 2) + chunks * (3 * others + 1) + 2 + 2 * others + 1
    return pl.pallas_call(
        functools.partial(kernel, n),
        out_shape=pltpu.VMEM((rows, out_weight.shape[1]), bf16),
        in_specs=[small, small] + [anywhere] * 6,
        out_specs=pl.BlockSpec(memory_space=pltpu.VMEM),
        scratch_shapes=[
            pltpu.VMEM((rows, depth), bf16),
            pltpu.VMEM((rows, depth), bf16),
            pltpu.VMEM((groups * depth, width), bf16),
            pltpu.VMEM((chunks * n * out_weight.shape[0], tile), bf16),
            pltpu.VMEM((n,) + chosen.shape, jnp.int32),
            pltpu.VMEM((total, width), bf16),
            pltpu.VMEM((n - 1, slots, width), bf16),
            pltpu.VMEM((rows, width), f32),
            pltpu.VMEM((rows, wide), f32),
            pltpu.VMEM((groups, rows, width), bf16),
            pltpu.VMEM((groups, rows, width), bf16),
            pltpu.VMEM((rows, wide), bf16),
            pltpu.VMEM((rows, total), f32),
            pltpu.VMEM((2, rows, wide), bf16),
            dma((4,)),
            dma((BULK + 2 * others + 1,)),
            dma((arrivals,)),
        ],
        compiler_params=pltpu.CompilerParams(
            collective_id=0, has_side_effects=True, vmem_limit_bytes=56 * 2**20
        ),
    )(chosen, live_length, tokens, query_weight, key_weight, value_weight, out_weight, chosen)


def solution(mesh):
    in_specs = (
        P(("dp", "kv"), None),
        P("kv", "tp"),
        P("kv", "tp"),
        P("kv", "tp"),
        P("kv", "tp"),
        P(("dp", "kv"), None),
        P("dp"),
    )
    out_specs = P(("dp", "kv"), "tp")
    fits = (mesh.shape["dp"], mesh.shape["kv"], mesh.shape["tp"]) == (4, 4, 2)
    body = woven_body if fits else gathered_body
    return jax.shard_map(body, mesh=mesh, in_specs=in_specs, out_specs=out_specs, check_vma=False)
```

```python
import collections
import functools
import math

import jax
import jax.numpy as jnp
from jax import lax
from jax.experimental import pallas as pl
from jax.experimental.pallas import tpu as pltpu
from jax.sharding import PartitionSpec as P

HD = 128
BLOCK = 32
CAP = 2
MESH = pl.DeviceIdType.MESH


def gathered_body(tokens, query_weight, key_weight, value_weight, out_weight, chosen, live_length):
    rows = tokens.shape[0]
    per_dev = rows // BLOCK
    owners = lax.axis_size("kv")
    me = lax.axis_index("kv")

    def add_rows(piece):
        return jnp.dot(tokens, piece, preferred_element_type=jnp.float32)

    queries = add_rows(lax.all_gather(query_weight, "kv", axis=0, tiled=True))
    keys = add_rows(lax.all_gather(key_weight, "kv", axis=0, tiled=True))
    values = add_rows(lax.all_gather(value_weight, "kv", axis=0, tiled=True))
    queries = queries.astype(jnp.bfloat16)
    paired = jnp.concatenate([keys.astype(jnp.bfloat16), values.astype(jnp.bfloat16)], axis=1)
    width = paired.shape[1]
    local_blocks = paired.reshape(per_dev, BLOCK, width)
    valid = chosen >= 0
    safe = jnp.maximum(chosen, 0)
    blocks_all = owners * per_dev
    hits = (safe[:, :, None] == jnp.arange(blocks_all, dtype=jnp.int32)[None, None, :]) & valid[
        :, :, None
    ]
    needed = jnp.any(hits, axis=(0, 1)).reshape(owners, per_dev)
    needed = needed & (jnp.arange(owners, dtype=jnp.int32) != me)[:, None]
    ranks = jnp.cumsum(needed.astype(jnp.int32), axis=1)
    local_ids = jnp.arange(per_dev, dtype=jnp.int32)
    slot_lists = []
    for slot in range(CAP):
        marked = needed & (ranks == slot + 1)
        found = jnp.any(marked, axis=1)
        where_at = jnp.sum(jnp.where(marked, local_ids[None, :], 0), axis=1)
        slot_lists.append(jnp.where(found, where_at, -1))
    wanted = jnp.stack(slot_lists, axis=1)
    requested = lax.all_to_all(wanted, "kv", split_axis=0, concat_axis=0, tiled=True)
    outgoing = local_blocks[jnp.maximum(requested, 0)]
    outgoing = jnp.where((requested >= 0)[:, :, None, None], outgoing, jnp.zeros((), jnp.bfloat16))
    incoming = lax.all_to_all(outgoing, "kv", split_axis=0, concat_axis=0, tiled=True)
    table = jnp.concatenate([incoming.reshape(owners * CAP, BLOCK, width), local_blocks], axis=0)
    segment_retainer = safe // per_dev
    local_of = safe % per_dev
    match = (wanted[None, None, :, :] == local_of[:, :, None, None]) & (
        jnp.arange(owners, dtype=jnp.int32)[None, None, :, None]
        == segment_retainer[:, :, None, None]
    )
    slot_index = jnp.arange(owners * CAP, dtype=jnp.int32).reshape(owners, CAP)
    remote_at = jnp.sum(jnp.where(match, slot_index[None, None], 0), axis=(2, 3))
    position = jnp.where(segment_retainer == me, owners * CAP + local_of, remote_at)
    picked = table[position]
    near_keys = picked[..., :HD]
    near_values = picked[..., HD:]
    grouped = queries.reshape(per_dev, BLOCK, -1, HD)
    scores = jnp.einsum(
        "jqhd,jnbd->jhqnb", grouped, near_keys, preferred_element_type=jnp.float32
    ) * HD ** (-0.5)
    query_pos = (me * per_dev + jnp.arange(per_dev, dtype=jnp.int32))[:, None] * BLOCK + jnp.arange(
        BLOCK, dtype=jnp.int32
    )[None, :]
    key_pos = safe[:, :, None] * BLOCK + jnp.arange(BLOCK, dtype=jnp.int32)[None, None, :]
    allowed = valid[:, None, :, None] & (key_pos[:, None, :, :] <= query_pos[:, :, None, None])
    masked = jnp.where(allowed[:, None], scores, -jnp.inf)
    top = jnp.max(masked, axis=(3, 4), keepdims=True)
    weights = jnp.exp(masked - top)
    total = jnp.sum(weights, axis=(3, 4))
    summed = jnp.einsum(
        "jhqnb,jnbd->jqhd",
        weights.astype(jnp.bfloat16),
        near_values,
        preferred_element_type=jnp.float32,
    )
    result = summed / jnp.transpose(total, (0, 2, 1))[..., None]
    live = query_pos < live_length[0]
    result = jnp.where(live[:, :, None, None], result, 0.0)
    attended = result.astype(jnp.bfloat16).reshape(rows, -1)
    every_head = lax.all_gather(attended, "tp", axis=1, tiled=True)
    mixed = jnp.dot(
        every_head,
        lax.all_gather(out_weight, "kv", axis=0, tiled=True),
        preferred_element_type=jnp.float32,
    )
    return mixed.astype(jnp.bfloat16)


HALF = 2
LEAST = 16
CUTS = {"q": 32, "p": 16}
MODES = "pppppphh"
SHARES = (2, 2, 2, 2, 2, 2, 2, 2)
HEADS = (2, 1, 1)
ORDER_END = (
    ("own", 0, 0), ("owno", 0, 0), ("owno", 4, 0), ("o", 2, 0), ("owno", 7, 0), ("o", 3, 0),
    ("own", 2, 0), ("own", 3, 0), ("owno", 6, 0), ("owno", 2, 0), ("w", 0, 0), ("o", 0, 0),
    ("ocy", 2, 0), ("owno", 5, 0), ("own", 1, 0), ("o", 2, 1), ("o", 5, 0), ("o", 3, 1),
    ("w", 1, 0), ("t", 0, 0), ("w", 0, 1), ("ocy", 5, 0), ("ocy", 0, 0), ("owno", 3, 0),
    ("ocy", 3, 1), ("w", 0, 2), ("o", 4, 0), ("o", 0, 1), ("o", 5, 1), ("o", 4, 2), ("ocy", 3, 0),
    ("o", 1, 0), ("owno", 1, 0), ("o", 1, 1), ("o", 4, 1), ("o", 5, 2), ("w", 1, 1),
    ("ocy", 1, 1), ("ocy", 2, 1), ("kv1", 0, 0), ("ocy", 5, 1), ("w", 1, 2), ("o", 0, 2),
    ("ocy", 4, 1), ("ocy", 4, 0), ("w", 3, 0), ("ocy", 4, 2), ("ocx", 5, 1), ("w", 3, 2),
    ("ocy", 0, 1), ("q1", 0, 0), ("ocy", 5, 2), ("ocx", 3, 0), ("w", 3, 1), ("w", 2, 0),
    ("ocx", 2, 1), ("ocx", 5, 0), ("ocy", 0, 2), ("w", 2, 1), ("kv2", 0, 0), ("w", 2, 2),
    ("ocy", 1, 0), ("o", 3, 2), ("ocx", 0, 2), ("ocx", 3, 1), ("o", 1, 2), ("ocx", 4, 0),
    ("q1", 2, 0), ("o", 7, 0), ("ocx", 1, 1), ("ocx", 5, 2), ("ocx", 4, 2), ("ocx", 4, 1),
    ("ocx", 1, 0), ("o", 2, 2), ("o", 6, 0), ("q1", 1, 0), ("ocy", 3, 2), ("q2", 2, 0),
    ("q2", 0, 0), ("ocx", 2, 0), ("ocx", 2, 2), ("ocx", 1, 2), ("ocx", 0, 1), ("ocx", 3, 2),
    ("ocy", 1, 2), ("o", 6, 2), ("att", 0, 0), ("o", 6, 1), ("q2", 1, 0), ("ocx", 0, 0),
    ("ocy", 2, 2), ("o", 7, 2), ("att", 1, 0), ("att", 2, 0), ("share", 0, 0), ("o", 7, 1),
    ("fin", 5, 0), ("fin", 4, 0), ("fin", 0, 0), ("fin", 3, 0), ("fin", 6, 0), ("fin", 2, 0),
    ("fin", 1, 0), ("fin", 7, 0),
)
ORDER_INNER = (
    ("owno", 3, 0), ("owno", 2, 0), ("own", 0, 0), ("owno", 0, 0), ("o", 3, 0), ("o", 2, 0),
    ("w", 0, 1), ("owno", 5, 0), ("own", 1, 0), ("w", 0, 0), ("w", 0, 2), ("owno", 4, 0),
    ("o", 0, 0), ("owno", 1, 0), ("o", 4, 1), ("o", 0, 1), ("o", 5, 1), ("o", 1, 0), ("o", 4, 2),
    ("o", 5, 0), ("w", 3, 1), ("w", 1, 1), ("o", 4, 0), ("t", 0, 0), ("o", 3, 1), ("o", 5, 2),
    ("ocy", 5, 1), ("kv1", 0, 0), ("w", 1, 0), ("ocy", 0, 0), ("ocx", 1, 0), ("w", 1, 2),
    ("ocy", 1, 0), ("own", 2, 0), ("o", 0, 2), ("own", 3, 0), ("ocy", 4, 0), ("w", 3, 2),
    ("ocy", 2, 0), ("w", 2, 1), ("w", 3, 0), ("o", 3, 2), ("w", 2, 0), ("ocx", 0, 2), ("o", 1, 1),
    ("ocy", 5, 2), ("w", 2, 2), ("ocy", 3, 1), ("o", 1, 2), ("ocy", 4, 2), ("ocx", 4, 0),
    ("owno", 6, 0), ("ocy", 3, 0), ("ocy", 0, 1), ("owno", 7, 0), ("ocx", 0, 0), ("o", 6, 1),
    ("ocx", 0, 1), ("q1", 0, 0), ("ocx", 1, 2), ("o", 2, 1), ("o", 2, 2), ("q1", 2, 0),
    ("ocx", 4, 1), ("o", 7, 1), ("ocx", 2, 0), ("ocy", 4, 1), ("kv2", 0, 0), ("ocx", 5, 1),
    ("o", 6, 2), ("q2", 0, 0), ("ocy", 5, 0), ("ocx", 3, 2), ("o", 6, 0), ("q1", 1, 0),
    ("ocy", 1, 2), ("o", 7, 2), ("o", 7, 0), ("ocx", 5, 2), ("ocy", 0, 2), ("att", 0, 0),
    ("q2", 1, 0), ("ocy", 3, 2), ("ocx", 2, 1), ("ocx", 1, 1), ("ocy", 1, 1), ("ocx", 5, 0),
    ("ocx", 3, 0), ("q2", 2, 0), ("ocx", 4, 2), ("att", 1, 0), ("att", 2, 0), ("ocy", 2, 2),
    ("ocx", 3, 1), ("ocx", 2, 2), ("share", 0, 0), ("ocy", 2, 1), ("fin", 0, 0), ("fin", 6, 0),
    ("fin", 1, 0), ("fin", 7, 0), ("fin", 5, 0), ("fin", 3, 0), ("fin", 4, 0), ("fin", 2, 0),
)


def pick(at, values):
    out = jnp.int32(values[0])
    for i, v in enumerate(values[1:]):
        out = jnp.where(at == i + 1, jnp.int32(v), out)
    return out


class Run:
    def __init__(self, ends):
        self.ends = ends
        self.sent = collections.defaultdict(int)

    def begin(self, c, kind, ref):
        c.start()
        self.sent[kind] += math.prod(ref.shape)


def kernel(
    n, tokens, query_w, key_w, value_w, out_w, listing, live_in, mixed,
    tok, other, weights, outs, lists, table, picked, mine_kv, mine_q, away, back,
    queries, bias, attended, chosen, live, local_sem, send_sem, recv_sem,
):
    dp, me, tp = lax.axis_index("dp"), lax.axis_index("kv"), lax.axis_index("tp")
    x_at, y_at = lax.rem(dp, 2), lax.div(dp, 2)
    right, left = jnp.minimum(me + 1, n - 1), jnp.maximum(me - 1, 0)
    to_x = {"dp": 2 * y_at + (1 - x_at)}
    to_y = {"dp": 2 * (1 - y_at) + x_at}
    dp_x, dp_y = 2 * y_at + (1 - x_at), 2 * (1 - y_at) + x_at
    dp_far = 2 * (1 - y_at) + (1 - x_at)
    side = lax.rem(x_at + y_at, 2)
    partner = {"tp": 1 - tp}
    rows = other.shape[0]
    depth = tok.shape[1]
    per_dev = rows // BLOCK
    seg = depth // n
    half_seg = seg // 2
    groups, chunks = len(weights), len(outs)
    widths = [ref.shape[1] for ref in weights]
    firsts = [sum(widths[1:g]) for g in range(groups)]
    tiles = [ref.shape[1] for ref in outs]
    owned = outs[0].shape[0] // n
    is_end = jnp.logical_or(me == 0, me == n - 1)
    inward = {"kv": jnp.where(me == 0, right, left)}
    near = [pick(me, v) for v in ((1, 2, 1, 2), (2, 0, 3, 1), (3, 3, 0, 0))]

    def load(src, dst, at):
        c = pltpu.make_async_copy(src, dst, local_sem.at[at])
        c.start()

    def loaded(ref, at):
        pltpu.make_async_copy(ref, ref, local_sem.at[at]).wait()

    def remote(src, dst, send, recv, target):
        return pltpu.make_async_remote_copy(
            src_ref=src, dst_ref=dst, send_sem=send_sem.at[send], recv_sem=recv_sem.at[recv],
            device_id=target, device_id_type=MESH,
        )

    def arrived(ref, recv):
        remote(ref, ref, 0, recv, partner).wait_recv()

    barrier = pltpu.get_barrier_semaphore()
    greeted = [{"kv": lax.rem(me + step, n)} for step in range(1, n)] + [to_x, to_y, partner]
    for target in greeted:
        pl.semaphore_signal(barrier, inc=1, device_id=target, device_id_type=MESH)

    my_rows = pl.ds(pl.multiple_of(x_at * seg, seg), seg)
    my_slab = pl.ds(pl.multiple_of(me * seg, seg), seg)
    for s in range(chunks):
        load(
            out_w.at[:, sum(tiles[:s]) : sum(tiles[: s + 1])],
            outs[s].at[pl.ds(pl.multiple_of(me * owned, owned), owned), :],
            groups + s,
        )
    load(key_w.at[my_rows, :], weights[0].at[my_slab, :HD], 0)
    load(value_w.at[my_rows, :], weights[0].at[my_slab, HD:], 0)
    for g in range(1, groups):
        load(
            query_w.at[my_rows, firsts[g] : firsts[g] + widths[g]], weights[g].at[my_slab, :], g
        )
    load(listing, lists.at[me], groups + chunks)
    load(listing, chosen, groups + chunks + 1)
    load(live_in, live, groups + chunks + 2)
    for k in range(n):
        load(
            tokens.at[:, pl.ds(pl.multiple_of((2 * k + x_at) * seg, seg), seg)],
            tok.at[:, k * seg : (k + 1) * seg],
            groups + chunks + 3,
        )

    with jax.named_scope("barrier"):
        pl.semaphore_wait(barrier, len(greeted))

    others = n - 1
    W = 0
    WY = W + groups * others
    O = WY + groups
    OX = O + chunks * others
    OY = OX + chunks * others
    OC = OY + chunks * others
    T = OC + chunks
    L = T + 2
    K = L + others
    Y = K + others
    S = Y + groups
    REST = groups + chunks
    FORTH, TOKENS, LISTS = REST + 1, REST + 2, REST + 3
    BLOCKS = LISTS + others

    def from_owner(owner, receiver):
        return lax.rem(owner + n - receiver, n) - 1

    my_part = pl.ds(pl.multiple_of(tp * (rows // 2), rows // 2), rows // 2)
    their_part = pl.ds(pl.multiple_of((1 - tp) * (rows // 2), rows // 2), rows // 2)
    for k in range(n):
        cols = pl.ds(pl.multiple_of((2 * k + 1 - x_at) * seg, seg), seg)
        remote(
            tokens.at[my_part, cols], other.at[my_part, k * seg : (k + 1) * seg], TOKENS, T, to_x
        ).start()

    def t_share(run):
        piece = other.at[my_part, :]
        arrived(piece, T)
        run.begin(remote(piece, piece, FORTH, T + 1, partner), FORTH, piece)

    def l_copy(step):
        return remote(
            listing, lists.at[me], LISTS + step - 1, L + step - 1, {"kv": jnp.maximum(me - step, 0)}
        )

    for step in range(1, n):
        pl.when(me >= step)(l_copy(step).start)

    def z_targets(run):
        return [inward] if run.ends else [{"kv": right}, {"kv": left}]

    def w_piece(group, owner, which):
        start = owner * seg + which * half_seg
        return weights[group].at[pl.ds(pl.multiple_of(start, half_seg), half_seg), :]

    def w_own(run, group):
        loaded(weights[group].at[:seg, :], group)
        piece = w_piece(group, me, y_at)
        for target in z_targets(run):
            recv = W + group * others + from_owner(me, target["kv"])
            run.begin(remote(piece, piece, group, recv, target), group, piece)

    def w_step(run, group, slot):
        owner = near[slot]
        piece = w_piece(group, owner, y_at)
        arrived(piece, W + group * others + from_owner(owner, me))
        if not run.ends:
            to = jnp.where(owner < me, right, left)
            recv = W + group * others + from_owner(owner, to)
            run.begin(remote(piece, piece, group, recv, {"kv": to}), group, piece)
        run.begin(remote(piece, piece, group, WY + group, to_y), group, piece)

    def w_arrive(group):
        arrived(weights[group].at[: others * half_seg, :], WY + group)

    quarter = owned // 4

    def o_piece(s, owner, first, size):
        return outs[s].at[pl.ds(pl.multiple_of(owner * owned + first, LEAST), size), :]

    def o_send(run, s, piece, recv, target):
        kind = groups + s
        run.begin(remote(piece, piece, kind, recv, target), kind, piece)

    def carried(s, owner):
        if MODES[s] in CUTS:
            return o_piece(s, owner, dp * quarter, quarter)
        return o_piece(s, owner, side * 2 * quarter, 2 * quarter)

    def o_own(run, s):
        loaded(outs[s].at[:owned, :], groups + s)
        for target in z_targets(run):
            o_send(run, s, carried(s, me), O + s * others + from_owner(me, target["kv"]), target)

    def o_step(run, s, slot):
        owner = near[slot]
        piece = carried(s, owner)
        arrived(piece, O + s * others + from_owner(owner, me))
        if not run.ends:
            to = jnp.where(owner < me, right, left)
            o_send(run, s, piece, O + s * others + from_owner(owner, to), {"kv": to})
        if MODES[s] in CUTS:
            at = s * others + from_owner(owner, me)
            o_send(run, s, piece, OX + at, to_x)
            o_send(run, s, piece, OY + at, to_y)
        else:
            o_send(run, s, o_piece(s, owner, 2 * side * quarter, quarter), OC + s, to_x)
            o_send(run, s, o_piece(s, owner, (2 * side + 1) * quarter, quarter), OC + s, to_y)

    def o_turn(run, s, slot, along_x):
        owner, cut = near[slot], CUTS[MODES[s]]
        at = s * others + from_owner(owner, me)
        if along_x:
            arrived(o_piece(s, owner, dp_x * quarter, quarter), OX + at)
            o_send(run, s, o_piece(s, owner, dp_x * quarter, cut), OC + s, to_y)
        else:
            arrived(o_piece(s, owner, dp_y * quarter, quarter), OY + at)
            o_send(run, s, o_piece(s, owner, dp_y * quarter + cut, quarter - cut), OC + s, to_x)

    def o_arrive(s):
        count = 1 if MODES[s] in CUTS else 2
        arrived(outs[s].at[: others * count * quarter, :], OC + s)

    def part(source, group):
        return jnp.dot(
            source[...], weights[group][...], preferred_element_type=jnp.float32
        )

    def y_copy(group):
        return remote(away[group], back[group], REST, Y + group, to_x)

    def project(run, group):
        w_arrive(group)
        away[group][...] = part(other, group).astype(jnp.bfloat16)
        run.begin(y_copy(group), REST, away[group])
        if group == 0:
            mine_kv[...] = part(tok, group)
        else:
            mine_q[:, firsts[group] : firsts[group] + widths[group]] = part(tok, group)

    slots = CAP * BLOCK
    local_at = n * slots

    def found(listed, block):
        return jnp.max((listed == block).astype(jnp.float32), axis=(0, 1), keepdims=True)

    def marks(listed, first):
        rank = jnp.zeros((1, 1), jnp.float32)
        out = [[] for _ in range(CAP)]
        for b in range(per_dev):
            one = found(listed, first + b)
            rank = rank + one
            for s in range(CAP):
                out[s].append(jnp.where(rank == s + 1, one, 0.0))
        return out

    def k_copy(step):
        return remote(
            picked.at[step - 1], table.at[pl.ds(pl.multiple_of(me * slots, slots), slots), :],
            BLOCKS + step - 1, K + step - 1, {"kv": jnp.minimum(me + step, n - 1)},
        )

    def k_arrive():
        for step in range(1, n):
            pl.when(me >= step)(k_copy(step).wait_recv)

    def share_blocks(run):
        y_copy(0).wait_recv()
        full = (mine_kv[...] + back[0][...].astype(jnp.float32)).astype(jnp.bfloat16)
        table[local_at : local_at + rows, :] = full
        full = full.astype(jnp.float32)
        for step in range(1, n):
            pl.when(me + step < n)(l_copy(step).wait_recv)
        for step in range(1, n):

            def send_to(step=step):
                which = marks(lists[me + step], me * per_dev)
                for s in range(CAP):
                    kept = jnp.zeros((BLOCK, full.shape[1]), jnp.float32)
                    for b in range(per_dev):
                        kept = kept + which[s][b] * full[b * BLOCK : (b + 1) * BLOCK, :]
                    picked[step - 1, s * BLOCK : (s + 1) * BLOCK, :] = kept.astype(jnp.bfloat16)

            pl.when(me + step < n)(send_to)
            pl.when(me + step < n)(k_copy(step).start)

    def build_bias():
        loaded(lists.at[me], groups + chunks)
        loaded(chosen, groups + chunks + 1)
        loaded(live, groups + chunks + 2)
        listed = lists[me]
        seq = bias.shape[1]
        column = lax.broadcasted_iota(jnp.int32, (8, seq), 1)
        block = me * per_dev + lax.div(column - local_at, BLOCK)
        for owner in range(n):
            which = marks(listed, owner * per_dev)
            for s in range(CAP):
                ident = jnp.full((1, 1), -2.0, jnp.float32)
                for b in range(per_dev):
                    ident = jnp.where(which[s][b] > 0.5, float(owner * per_dev + b), ident)
                ident = jnp.where(me == owner, -2.0, ident).astype(jnp.int32)
                block = jnp.where(lax.div(column, BLOCK) == owner * CAP + s, ident, block)
        at = block * BLOCK + lax.rem(column, BLOCK)
        at = jnp.concatenate([at] * (BLOCK // 8), axis=0)
        row = lax.broadcasted_iota(jnp.int32, (BLOCK, seq), 0)
        for j in range(per_dev):
            open_to = jnp.full((8, seq), -jnp.inf, jnp.float32)
            for e in range(chosen.shape[1]):
                open_to = jnp.where(block == chosen[j, e], 0.0, open_to)
            spread = jnp.concatenate([open_to] * (BLOCK // 8), axis=0)
            causal = at <= row + (me * rows + j * BLOCK)
            bias[j * BLOCK : (j + 1) * BLOCK, :] = jnp.where(causal, spread, -jnp.inf)

    def queries_done(group):
        y_copy(group).wait_recv()
        cols = slice(firsts[group], firsts[group] + widths[group])
        queries[:, cols] = (
            mine_q[:, cols] + back[group][...].astype(jnp.float32)
        ).astype(jnp.bfloat16)

    def attend(group):
        if group == 1:
            k_arrive()
        alive = me * rows + lax.broadcasted_iota(jnp.int32, (rows, HD), 0) < live[0]
        for h in range(firsts[group] // HD, (firsts[group] + widths[group]) // HD):
            cols = slice(h * HD, (h + 1) * HD)
            scores = lax.dot_general(
                queries[:, cols], table[:, :HD], (((1,), (1,)), ((), ())),
                preferred_element_type=jnp.float32,
            )
            masked = scores * HD ** (-0.5) + bias[...]
            top = jnp.max(masked, axis=1, keepdims=True)
            probs = jnp.exp(masked - top)
            total = jnp.sum(probs, axis=1, keepdims=True)
            summed = jnp.dot(
                probs.astype(jnp.bfloat16), table[:, HD:], preferred_element_type=jnp.float32
            )
            attended[tp, :, cols] = jnp.where(alive, summed / total, 0.0).astype(jnp.bfloat16)

    def share(run):
        piece = attended.at[tp]
        run.begin(remote(piece, piece, REST, S, partner), REST, piece)
        arrived(attended.at[1 - tp], S)

    wide = queries.shape[1]

    def final(s):
        o_arrive(s)
        acc = jnp.dot(
            attended[0], outs[s][:wide, :], preferred_element_type=jnp.float32
        )
        acc += jnp.dot(
            attended[1], outs[s][wide:, :], preferred_element_type=jnp.float32
        )
        mixed[:, sum(tiles[:s]) : sum(tiles[: s + 1])] = acc.astype(jnp.bfloat16)

    def settle():
        for owner in range(n):

            def clear(owner=owner):
                table[owner * slots : (owner + 1) * slots, :] = jnp.zeros(
                    (slots, table.shape[1]), table.dtype
                )

            pl.when(owner >= me)(clear)
        build_bias()
        loaded(tok, groups + chunks + 3)

    def act(run, name, i, j):
        if name == "own":
            w_own(run, i)
        elif name == "owno":
            o_own(run, i)
        elif name == "t":
            t_share(run)
        elif name == "w":
            w_step(run, i, j)
        elif name == "o":
            o_step(run, i, j)
        elif name == "ocx" or name == "ocy":
            o_turn(run, i, j, name == "ocx")
        elif name == "kv1":
            project(run, 0)
        elif name == "kv2":
            share_blocks(run)
        elif name == "q1":
            project(run, 1 + i)
        elif name == "q2":
            queries_done(1 + i)
        elif name == "att":
            attend(1 + i)
        elif name == "share":
            share(run)
        else:
            final(i)

    def follow(order, ends):
        run = Run(ends)
        begun = False
        projected = False
        for name, i, j in order:
            if not begun and not name.startswith("own"):
                settle()
                begun = True
            if not projected and name in ("kv1", "q1"):
                arrived(other.at[their_part, :], T + 1)
                projected = True
            with jax.named_scope(f"{name}_{i}_{j}"):
                act(run, name, i, j)
        for kind, size in run.sent.items():
            if kind < groups:
                ref = weights[kind].at[: size // widths[kind], :]
            elif kind < groups + chunks:
                ref = outs[kind - groups].at[: size // tiles[kind - groups], :]
            else:
                ref = tok.at[:, : size // rows]
            remote(ref, ref, kind, 0, partner).wait_send()

    pl.when(is_end)(functools.partial(follow, ORDER_END, True))
    pl.when(jnp.logical_not(is_end))(functools.partial(follow, ORDER_INNER, False))
    ref = other.at[my_part, :]
    remote(ref, ref, TOKENS, T, to_x).wait_send()
    for step in range(1, n):
        pl.when(me >= step)(l_copy(step).wait_send)
        pl.when(me + step < n)(k_copy(step).wait_send)


def woven_body(tokens, query_weight, key_weight, value_weight, out_weight, chosen, live_length):
    n = lax.axis_size("kv")
    rows, model = tokens.shape
    wide = query_weight.shape[1]
    depth = model // HALF
    width = 2 * HD
    widths = [width] + [heads * HD for heads in HEADS]
    unit = out_weight.shape[1] // sum(SHARES)
    tiles = [share * unit for share in SHARES]
    groups, chunks = len(widths), len(tiles)
    slots = CAP * BLOCK
    total = n * slots + rows
    dma = pltpu.SemaphoreType.DMA
    bf16 = jnp.bfloat16
    f32 = jnp.float32
    anywhere = pl.BlockSpec(memory_space=pl.ANY)
    others = n - 1
    arrivals = groups * (others + 2) + chunks * (3 * others + 1) + 2 + 2 * others + 1
    return pl.pallas_call(
        functools.partial(kernel, n),
        out_shape=pltpu.VMEM((rows, out_weight.shape[1]), bf16),
        in_specs=[anywhere] * 7,
        out_specs=pl.BlockSpec(memory_space=pltpu.VMEM),
        scratch_shapes=[
            pltpu.VMEM((rows, depth), bf16),
            pltpu.VMEM((rows, depth), bf16),
            tuple(pltpu.VMEM((depth, w), bf16) for w in widths),
            tuple(pltpu.VMEM((n * out_weight.shape[0], w), bf16) for w in tiles),
            pltpu.VMEM((n,) + chosen.shape, jnp.int32),
            pltpu.VMEM((total, width), bf16),
            pltpu.VMEM((n - 1, slots, width), bf16),
            pltpu.VMEM((rows, width), f32),
            pltpu.VMEM((rows, wide), f32),
            tuple(pltpu.VMEM((rows, w), bf16) for w in widths),
            tuple(pltpu.VMEM((rows, w), bf16) for w in widths),
            pltpu.VMEM((rows, wide), bf16),
            pltpu.VMEM((rows, total), f32),
            pltpu.VMEM((2, rows, wide), bf16),
            pltpu.SMEM(chosen.shape, jnp.int32),
            pltpu.SMEM(live_length.shape, jnp.int32),
            dma((groups + chunks + 4,)),
            dma((groups + chunks + 3 + 2 * others,)),
            dma((arrivals,)),
        ],
        compiler_params=pltpu.CompilerParams(
            collective_id=0, has_side_effects=True, vmem_limit_bytes=56 * 2**20
        ),
    )(tokens, query_weight, key_weight, value_weight, out_weight, chosen, live_length)


def solution(mesh):
    in_specs = (
        P(("dp", "kv"), None),
        P("kv", "tp"),
        P("kv", "tp"),
        P("kv", "tp"),
        P("kv", "tp"),
        P(("dp", "kv"), None),
        P("dp"),
    )
    out_specs = P(("dp", "kv"), "tp")
    fits = (mesh.shape["dp"], mesh.shape["kv"], mesh.shape["tp"]) == (4, 4, 2)
    body = woven_body if fits else gathered_body
    return jax.shard_map(body, mesh=mesh, in_specs=in_specs, out_specs=out_specs, check_vma=False)
```

```python
import collections
import functools
import math

import jax
import jax.numpy as jnp
from jax import lax
from jax.experimental import pallas as pl
from jax.experimental.pallas import tpu as pltpu
from jax.sharding import PartitionSpec as P

HD = 128
BLOCK = 32
CAP = 2
MESH = pl.DeviceIdType.MESH


def gathered_body(tokens, query_weight, key_weight, value_weight, out_weight, chosen, live_length):
    rows = tokens.shape[0]
    per_dev = rows // BLOCK
    owners = lax.axis_size("kv")
    me = lax.axis_index("kv")

    def add_rows(piece):
        return jnp.dot(tokens, piece, preferred_element_type=jnp.float32)

    queries = add_rows(lax.all_gather(query_weight, "kv", axis=0, tiled=True))
    keys = add_rows(lax.all_gather(key_weight, "kv", axis=0, tiled=True))
    values = add_rows(lax.all_gather(value_weight, "kv", axis=0, tiled=True))
    queries = queries.astype(jnp.bfloat16)
    paired = jnp.concatenate([keys.astype(jnp.bfloat16), values.astype(jnp.bfloat16)], axis=1)
    width = paired.shape[1]
    local_blocks = paired.reshape(per_dev, BLOCK, width)
    valid = chosen >= 0
    safe = jnp.maximum(chosen, 0)
    blocks_all = owners * per_dev
    hits = (safe[:, :, None] == jnp.arange(blocks_all, dtype=jnp.int32)[None, None, :]) & valid[
        :, :, None
    ]
    needed = jnp.any(hits, axis=(0, 1)).reshape(owners, per_dev)
    needed = needed & (jnp.arange(owners, dtype=jnp.int32) != me)[:, None]
    ranks = jnp.cumsum(needed.astype(jnp.int32), axis=1)
    local_ids = jnp.arange(per_dev, dtype=jnp.int32)
    slot_lists = []
    for slot in range(CAP):
        marked = needed & (ranks == slot + 1)
        found = jnp.any(marked, axis=1)
        where_at = jnp.sum(jnp.where(marked, local_ids[None, :], 0), axis=1)
        slot_lists.append(jnp.where(found, where_at, -1))
    wanted = jnp.stack(slot_lists, axis=1)
    requested = lax.all_to_all(wanted, "kv", split_axis=0, concat_axis=0, tiled=True)
    outgoing = local_blocks[jnp.maximum(requested, 0)]
    outgoing = jnp.where((requested >= 0)[:, :, None, None], outgoing, jnp.zeros((), jnp.bfloat16))
    incoming = lax.all_to_all(outgoing, "kv", split_axis=0, concat_axis=0, tiled=True)
    table = jnp.concatenate([incoming.reshape(owners * CAP, BLOCK, width), local_blocks], axis=0)
    segment_retainer = safe // per_dev
    local_of = safe % per_dev
    match = (wanted[None, None, :, :] == local_of[:, :, None, None]) & (
        jnp.arange(owners, dtype=jnp.int32)[None, None, :, None]
        == segment_retainer[:, :, None, None]
    )
    slot_index = jnp.arange(owners * CAP, dtype=jnp.int32).reshape(owners, CAP)
    remote_at = jnp.sum(jnp.where(match, slot_index[None, None], 0), axis=(2, 3))
    position = jnp.where(segment_retainer == me, owners * CAP + local_of, remote_at)
    picked = table[position]
    near_keys = picked[..., :HD]
    near_values = picked[..., HD:]
    grouped = queries.reshape(per_dev, BLOCK, -1, HD)
    scores = jnp.einsum(
        "jqhd,jnbd->jhqnb", grouped, near_keys, preferred_element_type=jnp.float32
    ) * HD ** (-0.5)
    query_pos = (me * per_dev + jnp.arange(per_dev, dtype=jnp.int32))[:, None] * BLOCK + jnp.arange(
        BLOCK, dtype=jnp.int32
    )[None, :]
    key_pos = safe[:, :, None] * BLOCK + jnp.arange(BLOCK, dtype=jnp.int32)[None, None, :]
    allowed = valid[:, None, :, None] & (key_pos[:, None, :, :] <= query_pos[:, :, None, None])
    masked = jnp.where(allowed[:, None], scores, -jnp.inf)
    top = jnp.max(masked, axis=(3, 4), keepdims=True)
    weights = jnp.exp(masked - top)
    total = jnp.sum(weights, axis=(3, 4))
    summed = jnp.einsum(
        "jhqnb,jnbd->jqhd",
        weights.astype(jnp.bfloat16),
        near_values,
        preferred_element_type=jnp.float32,
    )
    result = summed / jnp.transpose(total, (0, 2, 1))[..., None]
    live = query_pos < live_length[0]
    result = jnp.where(live[:, :, None, None], result, 0.0)
    attended = result.astype(jnp.bfloat16).reshape(rows, -1)
    every_head = lax.all_gather(attended, "tp", axis=1, tiled=True)
    mixed = jnp.dot(
        every_head,
        lax.all_gather(out_weight, "kv", axis=0, tiled=True),
        preferred_element_type=jnp.float32,
    )
    return mixed.astype(jnp.bfloat16)


HALF = 2
LEAST = 16
CUTS = {"q": 32, "p": 16}
MODES = "ppph"
SHARES = (4, 4, 4, 4)
HEADS = (2, 2)
ORDER_END = (
    ("owno", 2, 0), ("owno", 1, 0), ("owno", 0, 0), ("o", 2, 0), ("own", 0, 0), ("own", 2, 0),
    ("w", 0, 0), ("own", 1, 0), ("o", 1, 0), ("o", 2, 1), ("w", 0, 1), ("w", 1, 0),
    ("owno", 3, 0), ("ocy", 1, 0), ("o", 0, 0), ("t", 0, 0), ("ocy", 2, 1), ("o", 1, 1),
    ("o", 0, 2), ("o", 1, 2), ("w", 0, 2), ("ocy", 0, 2), ("o", 0, 1), ("ocy", 1, 2), ("w", 1, 2),
    ("w", 1, 1), ("ocy", 1, 1), ("ocy", 0, 0), ("w", 2, 0), ("ocy", 0, 1), ("kv1", 0, 0),
    ("w", 2, 1), ("q1", 0, 0), ("w", 2, 2), ("ocx", 2, 0), ("kv2", 0, 0), ("ocy", 2, 0),
    ("ocx", 1, 0), ("o", 2, 2), ("ocx", 0, 2), ("ocx", 0, 0), ("ocx", 1, 2), ("ocx", 0, 1),
    ("q2", 0, 0), ("ocx", 1, 1), ("o", 3, 0), ("q1", 1, 0), ("ocy", 2, 2), ("att", 0, 0),
    ("o", 3, 2), ("ocx", 2, 2), ("ocx", 2, 1), ("share", 0, 0), ("pre", 1, 0), ("o", 3, 1),
    ("q2", 1, 0), ("att", 1, 0), ("pre", 0, 0), ("share", 1, 0), ("pre", 2, 0), ("fin", 1, 0),
    ("fin", 0, 0), ("fin", 2, 0), ("pre", 3, 0), ("fin", 3, 0),
)
ORDER_INNER = (
    ("owno", 2, 0), ("own", 0, 0), ("o", 2, 0), ("owno", 1, 0), ("o", 1, 1), ("w", 0, 0),
    ("own", 1, 0), ("o", 0, 1), ("w", 0, 1), ("o", 1, 0), ("ocy", 2, 0), ("ocy", 1, 1),
    ("owno", 0, 0), ("ocy", 0, 1), ("t", 0, 0), ("w", 1, 1), ("o", 1, 2), ("o", 0, 2),
    ("w", 0, 2), ("o", 0, 0), ("w", 1, 2), ("w", 2, 1), ("w", 1, 0), ("own", 2, 0), ("ocy", 1, 0),
    ("o", 2, 1), ("w", 2, 0), ("w", 2, 2), ("ocy", 0, 0), ("o", 2, 2), ("o", 3, 1), ("ocx", 2, 0),
    ("ocx", 1, 2), ("kv1", 0, 0), ("ocy", 1, 2), ("ocx", 0, 0), ("owno", 3, 0), ("ocx", 0, 2),
    ("ocy", 2, 1), ("ocx", 1, 0), ("ocy", 0, 2), ("q1", 0, 0), ("kv2", 0, 0), ("ocx", 2, 2),
    ("o", 3, 2), ("ocx", 2, 1), ("q1", 1, 0), ("ocx", 1, 1), ("ocx", 0, 1), ("ocy", 2, 2),
    ("o", 3, 0), ("q2", 0, 0), ("att", 0, 0), ("share", 0, 0), ("q2", 1, 0), ("att", 1, 0),
    ("share", 1, 0), ("pre", 2, 0), ("pre", 0, 0), ("pre", 1, 0), ("fin", 2, 0), ("fin", 0, 0),
    ("pre", 3, 0), ("fin", 3, 0), ("fin", 1, 0),
)


def pick(at, values):
    out = jnp.int32(values[0])
    for i, v in enumerate(values[1:]):
        out = jnp.where(at == i + 1, jnp.int32(v), out)
    return out


class Run:
    def __init__(self, ends):
        self.ends = ends
        self.shared = 0
        self.sent = collections.defaultdict(int)

    def begin(self, c, kind, ref):
        c.start()
        self.sent[kind] += math.prod(ref.shape)


def kernel(
    n, tokens, query_w, key_w, value_w, out_w, listing, live_in, mixed,
    tok, other, weights, outs, lists, table, picked, mine_kv, mine_q, away, back,
    queries, bias, attended, summed, chosen, live, local_sem, send_sem, recv_sem,
):
    dp, me, tp = lax.axis_index("dp"), lax.axis_index("kv"), lax.axis_index("tp")
    x_at, y_at = lax.rem(dp, 2), lax.div(dp, 2)
    right, left = jnp.minimum(me + 1, n - 1), jnp.maximum(me - 1, 0)
    to_x = {"dp": 2 * y_at + (1 - x_at)}
    to_y = {"dp": 2 * (1 - y_at) + x_at}
    dp_x, dp_y = 2 * y_at + (1 - x_at), 2 * (1 - y_at) + x_at
    dp_far = 2 * (1 - y_at) + (1 - x_at)
    side = lax.rem(x_at + y_at, 2)
    partner = {"tp": 1 - tp}
    rows = other.shape[0]
    depth = tok.shape[1]
    per_dev = rows // BLOCK
    seg = depth // n
    half_seg = seg // 2
    groups, chunks = len(weights), len(outs)
    widths = [ref.shape[1] for ref in weights]
    firsts = [sum(widths[1:g]) for g in range(groups)]
    tiles = [ref.shape[1] for ref in outs]
    owned = outs[0].shape[0] // n
    is_end = jnp.logical_or(me == 0, me == n - 1)
    inward = {"kv": jnp.where(me == 0, right, left)}
    near = [pick(me, v) for v in ((1, 2, 1, 2), (2, 0, 3, 1), (3, 3, 0, 0))]

    def load(src, dst, at):
        c = pltpu.make_async_copy(src, dst, local_sem.at[at])
        c.start()

    def loaded(ref, at):
        pltpu.make_async_copy(ref, ref, local_sem.at[at]).wait()

    def remote(src, dst, send, recv, target):
        return pltpu.make_async_remote_copy(
            src_ref=src, dst_ref=dst, send_sem=send_sem.at[send], recv_sem=recv_sem.at[recv],
            device_id=target, device_id_type=MESH,
        )

    def arrived(ref, recv):
        remote(ref, ref, 0, recv, partner).wait_recv()

    barrier = pltpu.get_barrier_semaphore()

    def greet(target):
        pl.semaphore_signal(barrier, inc=1, device_id=target, device_id_type=MESH)

    pl.when(me < n - 1)(lambda: greet({"kv": right}))
    pl.when(me > 0)(lambda: greet({"kv": left}))
    for target in (to_x, to_y, partner):
        greet(target)

    my_rows = pl.ds(pl.multiple_of(x_at * seg, seg), seg)
    my_slab = pl.ds(pl.multiple_of(me * seg, seg), seg)
    for s in range(chunks):
        load(
            out_w.at[:, sum(tiles[:s]) : sum(tiles[: s + 1])],
            outs[s].at[pl.ds(pl.multiple_of(me * owned, owned), owned), :],
            groups + s,
        )
    load(key_w.at[my_rows, :], weights[0].at[my_slab, :HD], 0)
    load(value_w.at[my_rows, :], weights[0].at[my_slab, HD:], 0)
    for g in range(1, groups):
        load(
            query_w.at[my_rows, firsts[g] : firsts[g] + widths[g]], weights[g].at[my_slab, :], g
        )
    load(listing, lists.at[me], groups + chunks)
    load(listing, chosen, groups + chunks + 1)
    load(live_in, live, groups + chunks + 2)
    for k in range(n):
        load(
            tokens.at[:, pl.ds(pl.multiple_of((2 * k + x_at) * seg, seg), seg)],
            tok.at[:, k * seg : (k + 1) * seg],
            groups + chunks + 3,
        )

    with jax.named_scope("barrier"):
        pl.semaphore_wait(barrier, jnp.where(is_end, 4, 5))

    others = n - 1
    W = 0
    WY = W + groups * others
    O = WY + groups
    OX = O + chunks * others
    OY = OX + chunks * others
    OC = OY + chunks * others
    T = OC + chunks
    L = T + 2
    K = L + others
    Y = K + others
    S = Y + groups
    REST = groups + chunks
    FORTH, TOKENS, LISTS = REST + 1, REST + 2, REST + 3
    BLOCKS = LISTS + others

    def from_owner(owner, receiver):
        return lax.rem(owner + n - receiver, n) - 1

    my_part = pl.ds(pl.multiple_of(tp * (rows // 2), rows // 2), rows // 2)
    their_part = pl.ds(pl.multiple_of((1 - tp) * (rows // 2), rows // 2), rows // 2)
    for k in range(n):
        cols = pl.ds(pl.multiple_of((2 * k + 1 - x_at) * seg, seg), seg)
        remote(
            tokens.at[my_part, cols], other.at[my_part, k * seg : (k + 1) * seg], TOKENS, T, to_x
        ).start()

    def t_share(run):
        piece = other.at[my_part, :]
        arrived(piece, T)
        run.begin(remote(piece, piece, FORTH, T + 1, partner), FORTH, piece)

    def l_copy(step):
        return remote(
            listing, lists.at[me], LISTS + step - 1, L + step - 1, {"kv": jnp.maximum(me - step, 0)}
        )

    pl.when(me >= 1)(l_copy(1).start)

    def z_targets(run):
        return [inward] if run.ends else [{"kv": right}, {"kv": left}]

    def w_piece(group, owner, which):
        start = owner * seg + which * half_seg
        return weights[group].at[pl.ds(pl.multiple_of(start, half_seg), half_seg), :]

    def w_own(run, group):
        loaded(weights[group].at[:seg, :], group)
        piece = w_piece(group, me, y_at)
        for target in z_targets(run):
            recv = W + group * others + from_owner(me, target["kv"])
            run.begin(remote(piece, piece, group, recv, target), group, piece)

    def w_step(run, group, slot):
        owner = near[slot]
        piece = w_piece(group, owner, y_at)
        arrived(piece, W + group * others + from_owner(owner, me))
        if not run.ends:
            to = jnp.where(owner < me, right, left)
            recv = W + group * others + from_owner(owner, to)
            run.begin(remote(piece, piece, group, recv, {"kv": to}), group, piece)
        run.begin(remote(piece, piece, group, WY + group, to_y), group, piece)

    def w_arrive(group):
        arrived(weights[group].at[: others * half_seg, :], WY + group)

    quarter = owned // 4

    def o_piece(s, owner, first, size):
        return outs[s].at[pl.ds(pl.multiple_of(owner * owned + first, LEAST), size), :]

    def o_send(run, s, piece, recv, target):
        kind = groups + s
        run.begin(remote(piece, piece, kind, recv, target), kind, piece)

    def carried(s, owner):
        if MODES[s] in CUTS:
            return o_piece(s, owner, dp * quarter, quarter)
        return o_piece(s, owner, side * 2 * quarter, 2 * quarter)

    def o_own(run, s):
        loaded(outs[s].at[:owned, :], groups + s)
        for target in z_targets(run):
            o_send(run, s, carried(s, me), O + s * others + from_owner(me, target["kv"]), target)

    def o_step(run, s, slot):
        owner = near[slot]
        piece = carried(s, owner)
        arrived(piece, O + s * others + from_owner(owner, me))
        if not run.ends:
            to = jnp.where(owner < me, right, left)
            o_send(run, s, piece, O + s * others + from_owner(owner, to), {"kv": to})
        if MODES[s] in CUTS:
            at = s * others + from_owner(owner, me)
            o_send(run, s, piece, OX + at, to_x)
            o_send(run, s, piece, OY + at, to_y)
        else:
            o_send(run, s, o_piece(s, owner, 2 * side * quarter, quarter), OC + s, to_x)
            o_send(run, s, o_piece(s, owner, (2 * side + 1) * quarter, quarter), OC + s, to_y)

    def o_turn(run, s, slot, along_x):
        owner, cut = near[slot], CUTS[MODES[s]]
        at = s * others + from_owner(owner, me)
        if along_x:
            arrived(o_piece(s, owner, dp_x * quarter, quarter), OX + at)
            o_send(run, s, o_piece(s, owner, dp_x * quarter, cut), OC + s, to_y)
        else:
            arrived(o_piece(s, owner, dp_y * quarter, quarter), OY + at)
            o_send(run, s, o_piece(s, owner, dp_y * quarter + cut, quarter - cut), OC + s, to_x)

    def o_arrive(s):
        count = 1 if MODES[s] in CUTS else 2
        arrived(outs[s].at[: others * count * quarter, :], OC + s)

    def part(source, group):
        return jnp.dot(
            source[...], weights[group][...], preferred_element_type=jnp.float32
        )

    def y_copy(group):
        return remote(away[group], back[group], REST, Y + group, to_x)

    def project(run, group):
        w_arrive(group)
        away[group][...] = part(other, group).astype(jnp.bfloat16)
        run.begin(y_copy(group), REST, away[group])
        if group == 0:
            mine_kv[...] = part(tok, group)
        else:
            mine_q[:, firsts[group] : firsts[group] + widths[group]] = part(tok, group)

    slots = CAP * BLOCK
    local_at = n * slots

    def found(listed, block):
        return jnp.max((listed == block).astype(jnp.float32), axis=(0, 1), keepdims=True)

    def marks(listed, first):
        rank = jnp.zeros((1, 1), jnp.float32)
        out = [[] for _ in range(CAP)]
        for b in range(per_dev):
            one = found(listed, first + b)
            rank = rank + one
            for s in range(CAP):
                out[s].append(jnp.where(rank == s + 1, one, 0.0))
        return out

    def k_copy(step):
        return remote(
            picked.at[step - 1], table.at[pl.ds(pl.multiple_of(me * slots, slots), slots), :],
            BLOCKS + step - 1, K + step - 1, {"kv": jnp.minimum(me + step, n - 1)},
        )

    def k_arrive():
        for step in range(1, n):
            pl.when(me >= step)(k_copy(step).wait_recv)

    def share_blocks(run):
        y_copy(0).wait_recv()
        full = (mine_kv[...] + back[0][...].astype(jnp.float32)).astype(jnp.bfloat16)
        table[local_at : local_at + rows, :] = full
        full = full.astype(jnp.float32)
        for step in range(1, n):
            pl.when(me + step < n)(l_copy(step).wait_recv)
        for step in range(1, n):

            def send_to(step=step):
                which = marks(lists[me + step], me * per_dev)
                for s in range(CAP):
                    kept = jnp.zeros((BLOCK, full.shape[1]), jnp.float32)
                    for b in range(per_dev):
                        kept = kept + which[s][b] * full[b * BLOCK : (b + 1) * BLOCK, :]
                    picked[step - 1, s * BLOCK : (s + 1) * BLOCK, :] = kept.astype(jnp.bfloat16)

            pl.when(me + step < n)(send_to)
            pl.when(me + step < n)(k_copy(step).start)

    def build_bias():
        loaded(lists.at[me], groups + chunks)
        loaded(chosen, groups + chunks + 1)
        loaded(live, groups + chunks + 2)
        listed = lists[me]
        seq = bias.shape[1]
        column = lax.broadcasted_iota(jnp.int32, (8, seq), 1)
        block = me * per_dev + lax.div(column - local_at, BLOCK)
        for owner in range(n):
            which = marks(listed, owner * per_dev)
            for s in range(CAP):
                ident = jnp.full((1, 1), -2.0, jnp.float32)
                for b in range(per_dev):
                    ident = jnp.where(which[s][b] > 0.5, float(owner * per_dev + b), ident)
                ident = jnp.where(me == owner, -2.0, ident).astype(jnp.int32)
                block = jnp.where(lax.div(column, BLOCK) == owner * CAP + s, ident, block)
        at = block * BLOCK + lax.rem(column, BLOCK)
        at = jnp.concatenate([at] * (BLOCK // 8), axis=0)
        row = lax.broadcasted_iota(jnp.int32, (BLOCK, seq), 0)
        for j in range(per_dev):
            open_to = jnp.full((8, seq), -jnp.inf, jnp.float32)
            for e in range(chosen.shape[1]):
                open_to = jnp.where(block == chosen[j, e], 0.0, open_to)
            spread = jnp.concatenate([open_to] * (BLOCK // 8), axis=0)
            causal = at <= row + (me * rows + j * BLOCK)
            bias[j * BLOCK : (j + 1) * BLOCK, :] = jnp.where(causal, spread, -jnp.inf)

    def queries_done(group):
        y_copy(group).wait_recv()
        cols = slice(firsts[group], firsts[group] + widths[group])
        queries[:, cols] = (
            mine_q[:, cols] + back[group][...].astype(jnp.float32)
        ).astype(jnp.bfloat16)

    def attend(group):
        if group == 1:
            k_arrive()
        alive = me * rows + lax.broadcasted_iota(jnp.int32, (rows, HD), 0) < live[0]
        for h in range(firsts[group] // HD, (firsts[group] + widths[group]) // HD):
            cols = slice(h * HD, (h + 1) * HD)
            scores = lax.dot_general(
                queries[:, cols], table[:, :HD], (((1,), (1,)), ((), ())),
                preferred_element_type=jnp.float32,
            )
            masked = scores * HD ** (-0.5) + bias[...]
            top = jnp.max(masked, axis=1, keepdims=True)
            probs = jnp.exp(masked - top)
            total = jnp.sum(probs, axis=1, keepdims=True)
            summed = jnp.dot(
                probs.astype(jnp.bfloat16), table[:, HD:], preferred_element_type=jnp.float32
            )
            attended[tp, :, cols] = jnp.where(alive, summed / total, 0.0).astype(jnp.bfloat16)

    def of_group(which, group):
        return attended.at[which, :, firsts[group] : firsts[group] + widths[group]]

    def share(run, group):
        piece = of_group(tp, group)
        run.begin(remote(piece, piece, REST, S + group - 1, partner), REST, piece)

    def shared(run, last):
        while run.shared < last:
            run.shared += 1
            arrived(of_group(1 - tp, run.shared), S + run.shared - 1)

    wide = queries.shape[1]

    def mix(s, first, last):
        acc = jnp.zeros((rows, tiles[s]), jnp.float32)
        for which in range(2):
            acc += jnp.dot(
                attended[which, :, first:last],
                outs[s][which * wide + first : which * wide + last, :],
                preferred_element_type=jnp.float32,
            )
        return acc

    def early(run, s):
        shared(run, 1)
        o_arrive(s)
        summed[:, sum(tiles[:s]) : sum(tiles[: s + 1])] = mix(s, 0, widths[1])

    def final(run, s):
        shared(run, groups - 1)
        cols = slice(sum(tiles[:s]), sum(tiles[: s + 1]))
        mixed[:, cols] = (summed[:, cols] + mix(s, widths[1], wide)).astype(jnp.bfloat16)

    def settle():
        for owner in range(n):

            def clear(owner=owner):
                table[owner * slots : (owner + 1) * slots, :] = jnp.zeros(
                    (slots, table.shape[1]), table.dtype
                )

            pl.when(owner >= me)(clear)
        build_bias()
        loaded(tok, groups + chunks + 3)

    def act(run, name, i, j):
        if name == "own":
            w_own(run, i)
        elif name == "owno":
            o_own(run, i)
        elif name == "t":
            t_share(run)
        elif name == "w":
            w_step(run, i, j)
        elif name == "o":
            o_step(run, i, j)
        elif name == "ocx" or name == "ocy":
            o_turn(run, i, j, name == "ocx")
        elif name == "kv1":
            for step in range(2, n):
                pl.when(me >= step)(l_copy(step).start)
            project(run, 0)
        elif name == "kv2":
            share_blocks(run)
        elif name == "q1":
            project(run, 1 + i)
        elif name == "q2":
            queries_done(1 + i)
        elif name == "att":
            attend(1 + i)
        elif name == "share":
            share(run, 1 + i)
        elif name == "pre":
            early(run, i)
        else:
            final(run, i)

    def follow(order, ends):
        run = Run(ends)
        begun = False
        projected = False
        for name, i, j in order:
            if not begun and not name.startswith("own"):
                settle()
                begun = True
            if not projected and name in ("kv1", "q1"):
                arrived(other.at[their_part, :], T + 1)
                projected = True
            with jax.named_scope(f"{name}_{i}_{j}"):
                act(run, name, i, j)
        for kind, size in run.sent.items():
            if kind < groups:
                ref = weights[kind].at[: size // widths[kind], :]
            elif kind < groups + chunks:
                ref = outs[kind - groups].at[: size // tiles[kind - groups], :]
            else:
                ref = tok.at[:, : size // rows]
            remote(ref, ref, kind, 0, partner).wait_send()

    pl.when(is_end)(functools.partial(follow, ORDER_END, True))
    pl.when(jnp.logical_not(is_end))(functools.partial(follow, ORDER_INNER, False))
    ref = other.at[my_part, :]
    remote(ref, ref, TOKENS, T, to_x).wait_send()
    for step in range(1, n):
        pl.when(me >= step)(l_copy(step).wait_send)
        pl.when(me + step < n)(k_copy(step).wait_send)


def woven_body(tokens, query_weight, key_weight, value_weight, out_weight, chosen, live_length):
    n = lax.axis_size("kv")
    rows, model = tokens.shape
    wide = query_weight.shape[1]
    depth = model // HALF
    width = 2 * HD
    widths = [width] + [heads * HD for heads in HEADS]
    unit = out_weight.shape[1] // sum(SHARES)
    tiles = [share * unit for share in SHARES]
    groups, chunks = len(widths), len(tiles)
    slots = CAP * BLOCK
    total = n * slots + rows
    dma = pltpu.SemaphoreType.DMA
    bf16 = jnp.bfloat16
    f32 = jnp.float32
    anywhere = pl.BlockSpec(memory_space=pl.ANY)
    others = n - 1
    arrivals = groups * (others + 2) + chunks * (3 * others + 1) + 2 + 2 * others + groups - 1
    return pl.pallas_call(
        functools.partial(kernel, n),
        out_shape=pltpu.VMEM((rows, out_weight.shape[1]), bf16),
        in_specs=[anywhere] * 7,
        out_specs=pl.BlockSpec(memory_space=pltpu.VMEM),
        scratch_shapes=[
            pltpu.VMEM((rows, depth), bf16),
            pltpu.VMEM((rows, depth), bf16),
            tuple(pltpu.VMEM((depth, w), bf16) for w in widths),
            tuple(pltpu.VMEM((n * out_weight.shape[0], w), bf16) for w in tiles),
            pltpu.VMEM((n,) + chosen.shape, jnp.int32),
            pltpu.VMEM((total, width), bf16),
            pltpu.VMEM((n - 1, slots, width), bf16),
            pltpu.VMEM((rows, width), f32),
            pltpu.VMEM((rows, wide), f32),
            tuple(pltpu.VMEM((rows, w), bf16) for w in widths),
            tuple(pltpu.VMEM((rows, w), bf16) for w in widths),
            pltpu.VMEM((rows, wide), bf16),
            pltpu.VMEM((rows, total), f32),
            pltpu.VMEM((2, rows, wide), bf16),
            pltpu.VMEM((rows, out_weight.shape[1]), f32),
            pltpu.SMEM(chosen.shape, jnp.int32),
            pltpu.SMEM(live_length.shape, jnp.int32),
            dma((groups + chunks + 4,)),
            dma((groups + chunks + 3 + 2 * others,)),
            dma((arrivals,)),
        ],
        compiler_params=pltpu.CompilerParams(
            collective_id=0, has_side_effects=True, vmem_limit_bytes=56 * 2**20
        ),
    )(tokens, query_weight, key_weight, value_weight, out_weight, chosen, live_length)


def solution(mesh):
    in_specs = (
        P(("dp", "kv"), None),
        P("kv", "tp"),
        P("kv", "tp"),
        P("kv", "tp"),
        P("kv", "tp"),
        P(("dp", "kv"), None),
        P("dp"),
    )
    out_specs = P(("dp", "kv"), "tp")
    fits = (mesh.shape["dp"], mesh.shape["kv"], mesh.shape["tp"]) == (4, 4, 2)
    body = woven_body if fits else gathered_body
    return jax.shard_map(body, mesh=mesh, in_specs=in_specs, out_specs=out_specs, check_vma=False)
```

```python
import collections
import functools
import math

import jax
import jax.numpy as jnp
from jax import lax
from jax.experimental import pallas as pl
from jax.experimental.pallas import tpu as pltpu
from jax.sharding import PartitionSpec as P

HD = 128
BLOCK = 32
CAP = 2
MESH = pl.DeviceIdType.MESH


def gathered_body(tokens, query_weight, key_weight, value_weight, out_weight, chosen, live_length):
    rows = tokens.shape[0]
    per_dev = rows // BLOCK
    owners = lax.axis_size("kv")
    me = lax.axis_index("kv")

    def add_rows(piece):
        return jnp.dot(tokens, piece, preferred_element_type=jnp.float32)

    queries = add_rows(lax.all_gather(query_weight, "kv", axis=0, tiled=True))
    keys = add_rows(lax.all_gather(key_weight, "kv", axis=0, tiled=True))
    values = add_rows(lax.all_gather(value_weight, "kv", axis=0, tiled=True))
    queries = queries.astype(jnp.bfloat16)
    paired = jnp.concatenate([keys.astype(jnp.bfloat16), values.astype(jnp.bfloat16)], axis=1)
    width = paired.shape[1]
    local_blocks = paired.reshape(per_dev, BLOCK, width)
    valid = chosen >= 0
    safe = jnp.maximum(chosen, 0)
    blocks_all = owners * per_dev
    hits = (safe[:, :, None] == jnp.arange(blocks_all, dtype=jnp.int32)[None, None, :]) & valid[
        :, :, None
    ]
    needed = jnp.any(hits, axis=(0, 1)).reshape(owners, per_dev)
    needed = needed & (jnp.arange(owners, dtype=jnp.int32) != me)[:, None]
    ranks = jnp.cumsum(needed.astype(jnp.int32), axis=1)
    local_ids = jnp.arange(per_dev, dtype=jnp.int32)
    slot_lists = []
    for slot in range(CAP):
        marked = needed & (ranks == slot + 1)
        found = jnp.any(marked, axis=1)
        where_at = jnp.sum(jnp.where(marked, local_ids[None, :], 0), axis=1)
        slot_lists.append(jnp.where(found, where_at, -1))
    wanted = jnp.stack(slot_lists, axis=1)
    requested = lax.all_to_all(wanted, "kv", split_axis=0, concat_axis=0, tiled=True)
    outgoing = local_blocks[jnp.maximum(requested, 0)]
    outgoing = jnp.where((requested >= 0)[:, :, None, None], outgoing, jnp.zeros((), jnp.bfloat16))
    incoming = lax.all_to_all(outgoing, "kv", split_axis=0, concat_axis=0, tiled=True)
    table = jnp.concatenate([incoming.reshape(owners * CAP, BLOCK, width), local_blocks], axis=0)
    segment_retainer = safe // per_dev
    local_of = safe % per_dev
    match = (wanted[None, None, :, :] == local_of[:, :, None, None]) & (
        jnp.arange(owners, dtype=jnp.int32)[None, None, :, None]
        == segment_retainer[:, :, None, None]
    )
    slot_index = jnp.arange(owners * CAP, dtype=jnp.int32).reshape(owners, CAP)
    remote_at = jnp.sum(jnp.where(match, slot_index[None, None], 0), axis=(2, 3))
    position = jnp.where(segment_retainer == me, owners * CAP + local_of, remote_at)
    picked = table[position]
    near_keys = picked[..., :HD]
    near_values = picked[..., HD:]
    grouped = queries.reshape(per_dev, BLOCK, -1, HD)
    scores = jnp.einsum(
        "jqhd,jnbd->jhqnb", grouped, near_keys, preferred_element_type=jnp.float32
    ) * HD ** (-0.5)
    query_pos = (me * per_dev + jnp.arange(per_dev, dtype=jnp.int32))[:, None] * BLOCK + jnp.arange(
        BLOCK, dtype=jnp.int32
    )[None, :]
    key_pos = safe[:, :, None] * BLOCK + jnp.arange(BLOCK, dtype=jnp.int32)[None, None, :]
    allowed = valid[:, None, :, None] & (key_pos[:, None, :, :] <= query_pos[:, :, None, None])
    masked = jnp.where(allowed[:, None], scores, -jnp.inf)
    top = jnp.max(masked, axis=(3, 4), keepdims=True)
    weights = jnp.exp(masked - top)
    total = jnp.sum(weights, axis=(3, 4))
    summed = jnp.einsum(
        "jhqnb,jnbd->jqhd",
        weights.astype(jnp.bfloat16),
        near_values,
        preferred_element_type=jnp.float32,
    )
    result = summed / jnp.transpose(total, (0, 2, 1))[..., None]
    live = query_pos < live_length[0]
    result = jnp.where(live[:, :, None, None], result, 0.0)
    attended = result.astype(jnp.bfloat16).reshape(rows, -1)
    every_head = lax.all_gather(attended, "tp", axis=1, tiled=True)
    mixed = jnp.dot(
        every_head,
        lax.all_gather(out_weight, "kv", axis=0, tiled=True),
        preferred_element_type=jnp.float32,
    )
    return mixed.astype(jnp.bfloat16)


LEAST = 16
CUTS = {"q": 32, "p": 16, "s": 0}
MODES = "qqqh"
SHARES = (5, 4, 4, 3)
HEADS = (2, 1, 1)
ORDER_END = (
    ("owno", 0, 0), ("owno", 1, 0), ("o", 2, 0), ("own", 0, 0), ("owno", 2, 0), ("o", 1, 0),
    ("own", 2, 0), ("o", 2, 1), ("ocy", 2, 0), ("own", 1, 0), ("own", 3, 0), ("tf", 0, 0),
    ("ocy", 2, 1), ("ocx", 2, 0), ("o", 1, 1), ("o", 0, 2), ("ocx", 2, 1), ("ocy", 1, 0),
    ("w", 0, 0), ("owno", 3, 0), ("w", 0, 1), ("t", 0, 0), ("o", 1, 2), ("o", 0, 1),
    ("ocy", 0, 2), ("o", 0, 0), ("ocy", 1, 2), ("w", 0, 2), ("ocx", 1, 0), ("o", 2, 2),
    ("kv1", 0, 0), ("ocy", 1, 1), ("ocy", 0, 0), ("ocx", 0, 1), ("ocx", 0, 2), ("w", 2, 0),
    ("w", 1, 2), ("ocx", 1, 2), ("ocx", 1, 1), ("mid", 0, 0), ("ocx", 2, 2), ("w", 1, 1),
    ("w", 1, 0), ("ocy", 2, 2), ("q1", 0, 0), ("kv2", 0, 0), ("w", 2, 2), ("w", 2, 1),
    ("ocx", 0, 0), ("ocy", 0, 1), ("q1", 1, 0), ("w", 3, 2), ("mid", 1, 0), ("w", 3, 0),
    ("w", 3, 1), ("q1", 2, 0), ("mid", 2, 0), ("q2", 0, 0), ("o", 3, 0), ("att", 0, 0),
    ("mid", 3, 0), ("share", 0, 0), ("o", 3, 2), ("q2", 1, 0), ("att", 1, 0), ("share", 1, 0),
    ("pre", 1, 0), ("o", 3, 1), ("q2", 2, 0), ("att", 2, 0), ("share", 2, 0), ("pre", 2, 0),
    ("pre", 0, 0), ("fin", 2, 0), ("fin", 1, 0), ("pre", 3, 0), ("fin", 0, 0), ("fin", 3, 0),
)
ORDER_INNER = (
    ("owno", 2, 0), ("owno", 1, 0), ("own", 0, 0), ("o", 1, 1), ("o", 2, 0), ("o", 0, 1),
    ("owno", 0, 0), ("o", 1, 0), ("w", 0, 0), ("w", 0, 1), ("o", 2, 1), ("tf", 0, 0), ("o", 0, 2),
    ("o", 0, 0), ("o", 1, 2), ("w", 1, 1), ("w", 0, 2), ("own", 2, 0), ("o", 2, 2), ("w", 2, 1),
    ("t", 0, 0), ("ocy", 0, 1), ("own", 1, 0), ("ocy", 1, 1), ("o", 3, 1), ("ocx", 0, 0),
    ("w", 1, 2), ("kv1", 0, 0), ("w", 1, 0), ("ocx", 0, 1), ("w", 2, 0), ("ocx", 0, 2),
    ("w", 2, 2), ("ocx", 1, 1), ("own", 3, 0), ("ocy", 1, 2), ("q1", 1, 0), ("w", 3, 1),
    ("q1", 0, 0), ("w", 3, 2), ("w", 3, 0), ("ocy", 0, 2), ("ocy", 2, 2), ("mid", 0, 0),
    ("owno", 3, 0), ("ocx", 1, 2), ("q1", 2, 0), ("mid", 1, 0), ("kv2", 0, 0), ("mid", 2, 0),
    ("mid", 3, 0), ("ocx", 2, 1), ("o", 3, 2), ("o", 3, 0), ("q2", 1, 0), ("q2", 0, 0),
    ("ocy", 2, 0), ("q2", 2, 0), ("ocx", 1, 0), ("ocy", 0, 0), ("att", 0, 0), ("ocy", 1, 0),
    ("ocx", 2, 2), ("ocy", 2, 1), ("share", 0, 0), ("att", 1, 0), ("ocx", 2, 0), ("att", 2, 0),
    ("pre", 3, 0), ("share", 2, 0), ("share", 1, 0), ("pre", 0, 0), ("pre", 1, 0), ("fin", 1, 0),
    ("pre", 2, 0), ("fin", 0, 0), ("fin", 2, 0), ("fin", 3, 0),
)


def pick(at, values):
    out = jnp.int32(values[0])
    for i, v in enumerate(values[1:]):
        out = jnp.where(at == i + 1, jnp.int32(v), out)
    return out


class Run:
    def __init__(self, ends):
        self.ends = ends
        self.shared = 0
        self.projected = False
        self.sent = collections.defaultdict(int)

    def begin(self, c, kind, ref):
        c.start()
        self.sent[kind] += math.prod(ref.shape)


def kernel(
    n, tokens, query_w, key_w, value_w, out_w, listing, live_in, mixed,
    tok, other, crossing, held, weights, outs, lists, table, picked, mine, passing, away, back, away_on, back_on,
    queries, bias, attended, summed, chosen, live, local_sem, send_sem, recv_sem,
):
    dp, me, tp = lax.axis_index("dp"), lax.axis_index("kv"), lax.axis_index("tp")
    x_at, y_at = lax.rem(dp, 2), lax.div(dp, 2)
    right, left = jnp.minimum(me + 1, n - 1), jnp.maximum(me - 1, 0)
    to_x = {"dp": 2 * y_at + (1 - x_at)}
    to_y = {"dp": 2 * (1 - y_at) + x_at}
    dp_x, dp_y = 2 * y_at + (1 - x_at), 2 * (1 - y_at) + x_at
    dp_far = 2 * (1 - y_at) + (1 - x_at)
    side = lax.rem(x_at + y_at, 2)
    partner = {"tp": 1 - tp}
    to_far = {"dp": 2 * (1 - y_at) + (1 - x_at)}
    rows = tok.shape[0]
    depth = weights[0].shape[0]
    per_dev = rows // BLOCK
    seg = depth // n
    parts = 4
    groups, chunks = len(weights), len(outs)
    widths = [ref.shape[1] for ref in weights]
    firsts = [sum(widths[1:g]) for g in range(groups)]
    starts = [sum(widths[:g]) for g in range(groups)]
    tiles = [ref.shape[1] for ref in outs]
    owned = outs[0].shape[0] // n
    is_end = jnp.logical_or(me == 0, me == n - 1)
    inward = {"kv": jnp.where(me == 0, right, left)}
    near = [pick(me, v) for v in ((1, 2, 1, 2), (2, 0, 3, 1), (3, 3, 0, 0))]

    def load(src, dst, at):
        c = pltpu.make_async_copy(src, dst, local_sem.at[at])
        c.start()

    def loaded(ref, at):
        pltpu.make_async_copy(ref, ref, local_sem.at[at]).wait()

    def remote(src, dst, send, recv, target):
        return pltpu.make_async_remote_copy(
            src_ref=src, dst_ref=dst, send_sem=send_sem.at[send], recv_sem=recv_sem.at[recv],
            device_id=target, device_id_type=MESH,
        )

    def arrived(ref, recv):
        remote(ref, ref, 0, recv, partner).wait_recv()

    barrier = pltpu.get_barrier_semaphore()

    def greet(target):
        pl.semaphore_signal(barrier, inc=1, device_id=target, device_id_type=MESH)

    pl.when(me < n - 1)(lambda: greet({"kv": right}))
    pl.when(me > 0)(lambda: greet({"kv": left}))
    for target in (to_x, to_y, partner):
        greet(target)

    for s in range(chunks):
        load(
            out_w.at[:, sum(tiles[:s]) : sum(tiles[: s + 1])],
            outs[s].at[pl.ds(pl.multiple_of(me * owned, owned), owned), :],
            groups + s,
        )
    load(key_w, held[0].at[:, :HD], 0)
    load(value_w, held[0].at[:, HD:], 0)
    for g in range(1, groups):
        load(query_w.at[:, firsts[g] : firsts[g] + widths[g]], held[g], g)
    load(listing, lists.at[me], groups + chunks)
    load(listing, chosen, groups + chunks + 1)
    load(live_in, live, groups + chunks + 2)
    def token_cols(owner, index, count):
        return pl.ds(pl.multiple_of((parts * owner + index) * seg, seg), count * seg)

    for i, owner in enumerate(near):
        load(
            tokens.at[:, token_cols(owner, dp, 1)], tok.at[:, i * seg : (i + 1) * seg],
            groups + chunks + 3,
        )
    load(
        tokens.at[:, token_cols(me, 0, parts)], tok.at[:, (n - 1) * seg :], groups + chunks + 3
    )

    with jax.named_scope("barrier"):
        pl.semaphore_wait(barrier, jnp.where(is_end, 4, 5))

    others = n - 1
    W = 0
    O = W + groups * others
    OX = O + chunks * others
    OY = OX + chunks * others
    OC = OY + chunks * others
    T = OC + chunks
    L = T + 4
    K = L + others
    Y = K + others
    S = Y + 2 * groups
    REST = groups + chunks
    LATE, CROSS, FORTH, TOKENS, LISTS = (REST + 1 + i for i in range(5))
    BLOCKS = LISTS + others

    def from_owner(owner, receiver):
        return lax.rem(owner + n - receiver, n) - 1

    my_part = pl.ds(pl.multiple_of(tp * (rows // 2), rows // 2), rows // 2)
    their_part = pl.ds(pl.multiple_of((1 - tp) * (rows // 2), rows // 2), rows // 2)
    few = rows // 4
    first_rows = [pl.ds(pl.multiple_of(tp * (rows // 2) + i * few, few), few) for i in range(2)]

    def t_send(part, target, to, recv, via):
        for i, owner in enumerate(near):
            remote(
                tokens.at[part, token_cols(owner, target["dp"], 1)],
                to.at[:, i * seg : (i + 1) * seg], TOKENS, recv, via,
            ).start()

    t_send(my_part, to_x, other.at[0, my_part], T, to_x)
    t_send(my_part, to_y, other.at[1, my_part], T, to_y)
    t_send(first_rows[0], to_far, crossing.at[0], T + 2, to_x)
    t_send(first_rows[1], to_far, crossing.at[1], T + 3, to_y)

    def t_cross(run):
        for i, target in enumerate((to_y, to_x)):
            piece = crossing.at[i]
            arrived(piece, T + 2 + i)
            run.begin(
                remote(piece, other.at[2, first_rows[i]], CROSS, T, target), CROSS, piece
            )

    def t_share(run):
        piece = other.at[:, my_part, :]
        arrived(piece, T)
        run.begin(remote(piece, piece, FORTH, T + 1, partner), FORTH, piece)

    def l_copy(step):
        return remote(
            listing, lists.at[me], LISTS + step - 1, L + step - 1, {"kv": jnp.maximum(me - step, 0)}
        )

    pl.when(me >= 1)(l_copy(1).start)

    def z_targets(run):
        return [inward] if run.ends else [{"kv": right}, {"kv": left}]

    def w_piece(group, owner):
        return weights[group].at[pl.ds(pl.multiple_of(owner * seg, seg), seg), :]

    def w_own(run, group):
        loaded(held[group], group)
        source = held[group].at[pl.ds(pl.multiple_of(dp * seg, seg), seg), :]
        piece = w_piece(group, me)
        for target in z_targets(run):
            recv = W + group * others + from_owner(me, target["kv"])
            run.begin(remote(source, piece, group, recv, target), group, source)

    def w_step(run, group, slot):
        owner = near[slot]
        piece = w_piece(group, owner)
        arrived(piece, W + group * others + from_owner(owner, me))
        if not run.ends:
            to = jnp.where(owner < me, right, left)
            recv = W + group * others + from_owner(owner, to)
            run.begin(remote(piece, piece, group, recv, {"kv": to}), group, piece)

    quarter = owned // 4

    def o_piece(s, owner, first, size):
        return outs[s].at[pl.ds(pl.multiple_of(owner * owned + first, LEAST), size), :]

    def o_send(run, s, piece, recv, target):
        kind = groups + s
        run.begin(remote(piece, piece, kind, recv, target), kind, piece)

    def carried(s, owner):
        if MODES[s] in CUTS:
            return o_piece(s, owner, dp * quarter, quarter)
        return o_piece(s, owner, side * 2 * quarter, 2 * quarter)

    def o_own(run, s):
        loaded(outs[s].at[:owned, :], groups + s)
        for target in z_targets(run):
            o_send(run, s, carried(s, me), O + s * others + from_owner(me, target["kv"]), target)

    def o_step(run, s, slot):
        owner = near[slot]
        piece = carried(s, owner)
        arrived(piece, O + s * others + from_owner(owner, me))
        if not run.ends:
            to = jnp.where(owner < me, right, left)
            o_send(run, s, piece, O + s * others + from_owner(owner, to), {"kv": to})
        if MODES[s] in CUTS:
            at = s * others + from_owner(owner, me)
            o_send(run, s, piece, OX + at, to_x)
            o_send(run, s, piece, OY + at, to_y)
        else:
            o_send(run, s, o_piece(s, owner, 2 * side * quarter, quarter), OC + s, to_x)
            o_send(run, s, o_piece(s, owner, (2 * side + 1) * quarter, quarter), OC + s, to_y)

    def o_turn(run, s, slot, along_x):
        owner, cut = near[slot], CUTS[MODES[s]]
        at = s * others + from_owner(owner, me)
        if along_x:
            arrived(o_piece(s, owner, dp_x * quarter, quarter), OX + at)
            if cut:
                o_send(run, s, o_piece(s, owner, dp_x * quarter, cut), OC + s, to_y)
        else:
            arrived(o_piece(s, owner, dp_y * quarter, quarter), OY + at)
            o_send(run, s, o_piece(s, owner, dp_y * quarter + cut, quarter - cut), OC + s, to_x)

    def o_arrive(s):
        count = 1 if MODES[s] in CUTS else 2
        arrived(outs[s].at[: others * count * quarter, :], OC + s)

    def part(source, group):
        out = jnp.zeros((rows, widths[group]), jnp.float32)
        for i, owner in enumerate(near):
            slab = pl.ds(pl.multiple_of(owner * seg, seg), seg)
            out += jnp.dot(
                source[:, i * seg : (i + 1) * seg], weights[group][slab, :],
                preferred_element_type=jnp.float32,
            )
        return out

    def columns(group):
        return slice(starts[group], starts[group] + widths[group])

    def y_copy(group, along_y):
        return remote(
            away[along_y].at[:, columns(group)], back[along_y].at[:, columns(group)], REST,
            Y + 2 * group, to_y if along_y else to_x,
        )

    def on_copy(group, along_y):
        return remote(
            away_on[along_y].at[:, columns(group)], back_on[along_y].at[:, columns(group)], LATE,
            Y + 2 * group + 1, to_y if along_y else to_x,
        )

    def project(run, group):
        if not run.projected:
            arrived(other.at[:, their_part, :], T + 1)
            run.projected = True
        cols, half = columns(group), rows // 2
        far = part(other.at[2], group).astype(jnp.bfloat16)
        beside = part(other.at[0], group)
        above = part(other.at[1], group)
        away[0][:half, cols] = beside[:half].astype(jnp.bfloat16)
        away[0][half:, cols] = far[:half]
        away[1][:half, cols] = above[half:].astype(jnp.bfloat16)
        away[1][half:, cols] = far[half:]
        for along_y in range(2):
            run.begin(y_copy(group, along_y), REST, away[along_y].at[:, cols])
        passing[1, :, cols] = above[:half]
        passing[0, :, cols] = beside[half:]
        mine[:, cols] = part(tok, group) + jnp.dot(
            tok[:, (n - 1) * seg :], held[group][...], preferred_element_type=jnp.float32
        )

    def pass_on(run, group):
        cols, half = columns(group), rows // 2
        arrived(tok.at[:, : 2 * widths[group]], Y + 2 * group)
        for along_y in (1, 0):
            took = back[1 - along_y][half:, cols].astype(jnp.float32)
            away_on[along_y][:, cols] = (passing[along_y, :, cols] + took).astype(jnp.bfloat16)
            run.begin(on_copy(group, along_y), LATE, away_on[along_y].at[:, cols])

    def collected(group):
        cols, half = columns(group), rows // 2
        arrived(tok.at[:, : widths[group]], Y + 2 * group + 1)
        halves = []
        for i, along_y in enumerate((1, 0)):
            halves.append(
                mine[i * half : (i + 1) * half, cols]
                + back[1 - along_y][:half, cols].astype(jnp.float32)
                + back_on[along_y][:, cols].astype(jnp.float32)
            )
        return jnp.concatenate(halves, axis=0).astype(jnp.bfloat16)

    slots = CAP * BLOCK
    local_at = n * slots

    def found(listed, block):
        return jnp.max((listed == block).astype(jnp.float32), axis=(0, 1), keepdims=True)

    def marks(listed, first):
        rank = jnp.zeros((1, 1), jnp.float32)
        out = [[] for _ in range(CAP)]
        for b in range(per_dev):
            one = found(listed, first + b)
            rank = rank + one
            for s in range(CAP):
                out[s].append(jnp.where(rank == s + 1, one, 0.0))
        return out

    def k_copy(step):
        return remote(
            picked.at[step - 1], table.at[pl.ds(pl.multiple_of(me * slots, slots), slots), :],
            BLOCKS + step - 1, K + step - 1, {"kv": jnp.minimum(me + step, n - 1)},
        )

    def k_arrive():
        for step in range(1, n):
            pl.when(me >= step)(k_copy(step).wait_recv)

    def share_blocks(run):
        full = collected(0)
        table[local_at : local_at + rows, :] = full
        full = full.astype(jnp.float32)
        for step in range(1, n):
            pl.when(me + step < n)(l_copy(step).wait_recv)
        for step in range(1, n):

            def send_to(step=step):
                which = marks(lists[me + step], me * per_dev)
                for s in range(CAP):
                    kept = jnp.zeros((BLOCK, full.shape[1]), jnp.float32)
                    for b in range(per_dev):
                        kept = kept + which[s][b] * full[b * BLOCK : (b + 1) * BLOCK, :]
                    picked[step - 1, s * BLOCK : (s + 1) * BLOCK, :] = kept.astype(jnp.bfloat16)

            pl.when(me + step < n)(send_to)
            pl.when(me + step < n)(k_copy(step).start)

    def build_bias():
        loaded(lists.at[me], groups + chunks)
        loaded(chosen, groups + chunks + 1)
        loaded(live, groups + chunks + 2)
        listed = lists[me]
        seq = bias.shape[1]
        column = lax.broadcasted_iota(jnp.int32, (8, seq), 1)
        block = me * per_dev + lax.div(column - local_at, BLOCK)
        for owner in range(n):
            which = marks(listed, owner * per_dev)
            for s in range(CAP):
                ident = jnp.full((1, 1), -2.0, jnp.float32)
                for b in range(per_dev):
                    ident = jnp.where(which[s][b] > 0.5, float(owner * per_dev + b), ident)
                ident = jnp.where(me == owner, -2.0, ident).astype(jnp.int32)
                block = jnp.where(lax.div(column, BLOCK) == owner * CAP + s, ident, block)
        at = block * BLOCK + lax.rem(column, BLOCK)
        at = jnp.concatenate([at] * (BLOCK // 8), axis=0)
        row = lax.broadcasted_iota(jnp.int32, (BLOCK, seq), 0)
        for j in range(per_dev):
            open_to = jnp.full((8, seq), -jnp.inf, jnp.float32)
            for e in range(chosen.shape[1]):
                open_to = jnp.where(block == chosen[j, e], 0.0, open_to)
            spread = jnp.concatenate([open_to] * (BLOCK // 8), axis=0)
            causal = at <= row + (me * rows + j * BLOCK)
            bias[j * BLOCK : (j + 1) * BLOCK, :] = jnp.where(causal, spread, -jnp.inf)

    def queries_done(group):
        queries[:, firsts[group] : firsts[group] + widths[group]] = collected(group)

    def attend(group):
        if group == 1:
            k_arrive()
        alive = me * rows + lax.broadcasted_iota(jnp.int32, (rows, HD), 0) < live[0]
        for h in range(firsts[group] // HD, (firsts[group] + widths[group]) // HD):
            cols = slice(h * HD, (h + 1) * HD)
            scores = lax.dot_general(
                queries[:, cols], table[:, :HD], (((1,), (1,)), ((), ())),
                preferred_element_type=jnp.float32,
            )
            masked = scores * HD ** (-0.5) + bias[...]
            top = jnp.max(masked, axis=1, keepdims=True)
            probs = jnp.exp(masked - top)
            total = jnp.sum(probs, axis=1, keepdims=True)
            summed = jnp.dot(
                probs.astype(jnp.bfloat16), table[:, HD:], preferred_element_type=jnp.float32
            )
            attended[tp, :, cols] = jnp.where(alive, summed / total, 0.0).astype(jnp.bfloat16)

    def of_group(which, group):
        return attended.at[which, :, firsts[group] : firsts[group] + widths[group]]

    def share(run, group):
        piece = of_group(tp, group)
        run.begin(remote(piece, piece, LATE, S + group - 1, partner), LATE, piece)

    def shared(run, last):
        while run.shared < last:
            run.shared += 1
            arrived(of_group(1 - tp, run.shared), S + run.shared - 1)

    wide = queries.shape[1]

    def mix(s, first, last):
        acc = jnp.zeros((rows, tiles[s]), jnp.float32)
        for which in range(2):
            acc += jnp.dot(
                attended[which, :, first:last],
                outs[s][which * wide + first : which * wide + last, :],
                preferred_element_type=jnp.float32,
            )
        return acc

    def early(run, s):
        shared(run, 1)
        o_arrive(s)
        summed[:, sum(tiles[:s]) : sum(tiles[: s + 1])] = mix(s, 0, widths[1])

    def final(run, s):
        shared(run, groups - 1)
        cols = slice(sum(tiles[:s]), sum(tiles[: s + 1]))
        mixed[:, cols] = (summed[:, cols] + mix(s, widths[1], wide)).astype(jnp.bfloat16)

    def settle():
        for owner in range(n):

            def clear(owner=owner):
                table[owner * slots : (owner + 1) * slots, :] = jnp.zeros(
                    (slots, table.shape[1]), table.dtype
                )

            pl.when(owner >= me)(clear)
        build_bias()
        loaded(tok, groups + chunks + 3)

    def act(run, name, i, j):
        if name == "own":
            w_own(run, i)
        elif name == "owno":
            o_own(run, i)
        elif name == "t":
            t_share(run)
        elif name == "tf":
            t_cross(run)
        elif name == "w":
            w_step(run, i, j)
        elif name == "o":
            o_step(run, i, j)
        elif name == "ocx" or name == "ocy":
            o_turn(run, i, j, name == "ocx")
        elif name == "kv1":
            for step in range(2, n):
                pl.when(me >= step)(l_copy(step).start)
            project(run, 0)
        elif name == "mid":
            pass_on(run, i)
        elif name == "kv2":
            share_blocks(run)
        elif name == "q1":
            project(run, 1 + i)
        elif name == "q2":
            queries_done(1 + i)
        elif name == "att":
            attend(1 + i)
        elif name == "share":
            share(run, 1 + i)
        elif name == "pre":
            early(run, i)
        else:
            final(run, i)

    def follow(order, ends):
        run = Run(ends)
        begun = False
        for name, i, j in order:
            if not begun and not name.startswith("own"):
                settle()
                begun = True
            with jax.named_scope(f"{name}_{i}_{j}"):
                act(run, name, i, j)
        for kind, size in run.sent.items():
            if groups <= kind < groups + chunks:
                ref = outs[kind - groups].at[: size // tiles[kind - groups], :]
            elif kind < groups or kind in (REST, LATE):
                ref = tok.at[:, : size // rows]
            elif kind == CROSS:
                ref = crossing
            else:
                ref = other.at[:, my_part, :]
            remote(ref, ref, kind, 0, partner).wait_send()

    pl.when(is_end)(functools.partial(follow, ORDER_END, True))
    pl.when(jnp.logical_not(is_end))(functools.partial(follow, ORDER_INNER, False))
    ref = other.at[:, my_part, :]
    remote(ref, ref, TOKENS, T, to_x).wait_send()
    for step in range(1, n):
        pl.when(me >= step)(l_copy(step).wait_send)
        pl.when(me + step < n)(k_copy(step).wait_send)


def woven_body(tokens, query_weight, key_weight, value_weight, out_weight, chosen, live_length):
    n = lax.axis_size("kv")
    rows, model = tokens.shape
    wide = query_weight.shape[1]
    seg = model // n // 4
    width = 2 * HD
    widths = [width] + [heads * HD for heads in HEADS]
    unit = out_weight.shape[1] // sum(SHARES)
    tiles = [share * unit for share in SHARES]
    groups, chunks = len(widths), len(tiles)
    every = sum(widths)
    slots = CAP * BLOCK
    total = n * slots + rows
    dma = pltpu.SemaphoreType.DMA
    bf16 = jnp.bfloat16
    f32 = jnp.float32
    anywhere = pl.BlockSpec(memory_space=pl.ANY)
    others = n - 1
    arrivals = groups * (others + 2) + chunks * (3 * others + 1) + 4 + 2 * others + groups - 1
    return pl.pallas_call(
        functools.partial(kernel, n),
        out_shape=pltpu.VMEM((rows, out_weight.shape[1]), bf16),
        in_specs=[anywhere] * 7,
        out_specs=pl.BlockSpec(memory_space=pltpu.VMEM),
        scratch_shapes=[
            pltpu.VMEM((rows, (n - 1) * seg + model // n), bf16),
            pltpu.VMEM((3, rows, (n - 1) * seg), bf16),
            pltpu.VMEM((2, rows // 4, (n - 1) * seg), bf16),
            tuple(pltpu.VMEM((key_weight.shape[0], w), bf16) for w in widths),
            tuple(pltpu.VMEM((n * seg, w), bf16) for w in widths),
            tuple(pltpu.VMEM((n * out_weight.shape[0], w), bf16) for w in tiles),
            pltpu.VMEM((n,) + chosen.shape, jnp.int32),
            pltpu.VMEM((total, width), bf16),
            pltpu.VMEM((n - 1, slots, width), bf16),
            pltpu.VMEM((rows, every), f32),
            pltpu.VMEM((2, rows // 2, every), f32),
            tuple(pltpu.VMEM((rows, every), bf16) for _ in range(2)),
            tuple(pltpu.VMEM((rows, every), bf16) for _ in range(2)),
            tuple(pltpu.VMEM((rows // 2, every), bf16) for _ in range(2)),
            tuple(pltpu.VMEM((rows // 2, every), bf16) for _ in range(2)),
            pltpu.VMEM((rows, wide), bf16),
            pltpu.VMEM((rows, total), f32),
            pltpu.VMEM((2, rows, wide), bf16),
            pltpu.VMEM((rows, out_weight.shape[1]), f32),
            pltpu.SMEM(chosen.shape, jnp.int32),
            pltpu.SMEM(live_length.shape, jnp.int32),
            dma((groups + chunks + 4,)),
            dma((groups + chunks + 5 + 2 * others,)),
            dma((arrivals,)),
        ],
        compiler_params=pltpu.CompilerParams(
            collective_id=0, has_side_effects=True, vmem_limit_bytes=56 * 2**20
        ),
    )(tokens, query_weight, key_weight, value_weight, out_weight, chosen, live_length)


def solution(mesh):
    in_specs = (
        P(("dp", "kv"), None),
        P("kv", "tp"),
        P("kv", "tp"),
        P("kv", "tp"),
        P("kv", "tp"),
        P(("dp", "kv"), None),
        P("dp"),
    )
    out_specs = P(("dp", "kv"), "tp")
    fits = (mesh.shape["dp"], mesh.shape["kv"], mesh.shape["tp"]) == (4, 4, 2)
    body = woven_body if fits else gathered_body
    return jax.shard_map(body, mesh=mesh, in_specs=in_specs, out_specs=out_specs, check_vma=False)
```

```python
import collections
import functools
import math

import jax
import jax.numpy as jnp
from jax import lax
from jax.experimental import pallas as pl
from jax.experimental.pallas import tpu as pltpu
from jax.sharding import PartitionSpec as P

HD = 128
BLOCK = 32
CAP = 2
MESH = pl.DeviceIdType.MESH


def gathered_body(tokens, query_weight, key_weight, value_weight, out_weight, chosen, live_length):
    rows = tokens.shape[0]
    per_dev = rows // BLOCK
    owners = lax.axis_size("kv")
    me = lax.axis_index("kv")

    def add_rows(piece):
        return jnp.dot(tokens, piece, preferred_element_type=jnp.float32)

    queries = add_rows(lax.all_gather(query_weight, "kv", axis=0, tiled=True))
    keys = add_rows(lax.all_gather(key_weight, "kv", axis=0, tiled=True))
    values = add_rows(lax.all_gather(value_weight, "kv", axis=0, tiled=True))
    queries = queries.astype(jnp.bfloat16)
    paired = jnp.concatenate([keys.astype(jnp.bfloat16), values.astype(jnp.bfloat16)], axis=1)
    width = paired.shape[1]
    local_blocks = paired.reshape(per_dev, BLOCK, width)
    valid = chosen >= 0
    safe = jnp.maximum(chosen, 0)
    blocks_all = owners * per_dev
    hits = (safe[:, :, None] == jnp.arange(blocks_all, dtype=jnp.int32)[None, None, :]) & valid[
        :, :, None
    ]
    needed = jnp.any(hits, axis=(0, 1)).reshape(owners, per_dev)
    needed = needed & (jnp.arange(owners, dtype=jnp.int32) != me)[:, None]
    ranks = jnp.cumsum(needed.astype(jnp.int32), axis=1)
    local_ids = jnp.arange(per_dev, dtype=jnp.int32)
    slot_lists = []
    for slot in range(CAP):
        marked = needed & (ranks == slot + 1)
        found = jnp.any(marked, axis=1)
        where_at = jnp.sum(jnp.where(marked, local_ids[None, :], 0), axis=1)
        slot_lists.append(jnp.where(found, where_at, -1))
    wanted = jnp.stack(slot_lists, axis=1)
    requested = lax.all_to_all(wanted, "kv", split_axis=0, concat_axis=0, tiled=True)
    outgoing = local_blocks[jnp.maximum(requested, 0)]
    outgoing = jnp.where((requested >= 0)[:, :, None, None], outgoing, jnp.zeros((), jnp.bfloat16))
    incoming = lax.all_to_all(outgoing, "kv", split_axis=0, concat_axis=0, tiled=True)
    table = jnp.concatenate([incoming.reshape(owners * CAP, BLOCK, width), local_blocks], axis=0)
    segment_retainer = safe // per_dev
    local_of = safe % per_dev
    match = (wanted[None, None, :, :] == local_of[:, :, None, None]) & (
        jnp.arange(owners, dtype=jnp.int32)[None, None, :, None]
        == segment_retainer[:, :, None, None]
    )
    slot_index = jnp.arange(owners * CAP, dtype=jnp.int32).reshape(owners, CAP)
    remote_at = jnp.sum(jnp.where(match, slot_index[None, None], 0), axis=(2, 3))
    position = jnp.where(segment_retainer == me, owners * CAP + local_of, remote_at)
    picked = table[position]
    near_keys = picked[..., :HD]
    near_values = picked[..., HD:]
    grouped = queries.reshape(per_dev, BLOCK, -1, HD)
    scores = jnp.einsum(
        "jqhd,jnbd->jhqnb", grouped, near_keys, preferred_element_type=jnp.float32
    ) * HD ** (-0.5)
    query_pos = (me * per_dev + jnp.arange(per_dev, dtype=jnp.int32))[:, None] * BLOCK + jnp.arange(
        BLOCK, dtype=jnp.int32
    )[None, :]
    key_pos = safe[:, :, None] * BLOCK + jnp.arange(BLOCK, dtype=jnp.int32)[None, None, :]
    allowed = valid[:, None, :, None] & (key_pos[:, None, :, :] <= query_pos[:, :, None, None])
    masked = jnp.where(allowed[:, None], scores, -jnp.inf)
    top = jnp.max(masked, axis=(3, 4), keepdims=True)
    weights = jnp.exp(masked - top)
    total = jnp.sum(weights, axis=(3, 4))
    summed = jnp.einsum(
        "jhqnb,jnbd->jqhd",
        weights.astype(jnp.bfloat16),
        near_values,
        preferred_element_type=jnp.float32,
    )
    result = summed / jnp.transpose(total, (0, 2, 1))[..., None]
    live = query_pos < live_length[0]
    result = jnp.where(live[:, :, None, None], result, 0.0)
    attended = result.astype(jnp.bfloat16).reshape(rows, -1)
    every_head = lax.all_gather(attended, "tp", axis=1, tiled=True)
    mixed = jnp.dot(
        every_head,
        lax.all_gather(out_weight, "kv", axis=0, tiled=True),
        preferred_element_type=jnp.float32,
    )
    return mixed.astype(jnp.bfloat16)


LEAST = 16
CUTS = {"q": 32, "p": 16, "s": 0}
MODES = "qqqh"
SHARES = (5, 4, 4, 3)
HEADS = (2, 1, 1)
ORDER_END = (
    ("owno", 0, 0), ("owno", 1, 0), ("o", 2, 0), ("own", 0, 0), ("owno", 2, 0), ("o", 1, 0),
    ("own", 2, 0), ("o", 2, 1), ("ocy", 2, 0), ("own", 1, 0), ("own", 3, 0), ("tf", 0, 0),
    ("ocy", 2, 1), ("ocx", 2, 0), ("o", 1, 1), ("o", 0, 2), ("ocx", 2, 1), ("ocy", 1, 0),
    ("w", 0, 0), ("owno", 3, 0), ("w", 0, 1), ("t", 0, 0), ("o", 1, 2), ("o", 0, 1),
    ("ocy", 0, 2), ("o", 0, 0), ("ocy", 1, 2), ("w", 0, 2), ("ocx", 1, 0), ("o", 2, 2),
    ("kv1", 0, 0), ("ocy", 1, 1), ("ocy", 0, 0), ("ocx", 0, 1), ("ocx", 0, 2), ("w", 2, 0),
    ("w", 1, 2), ("ocx", 1, 2), ("ocx", 1, 1), ("mid", 0, 0), ("ocx", 2, 2), ("w", 1, 1),
    ("w", 1, 0), ("ocy", 2, 2), ("q1", 0, 0), ("kv2", 0, 0), ("w", 2, 2), ("w", 2, 1),
    ("ocx", 0, 0), ("ocy", 0, 1), ("q1", 1, 0), ("w", 3, 2), ("mid", 1, 0), ("w", 3, 0),
    ("w", 3, 1), ("q1", 2, 0), ("mid", 2, 0), ("q2", 0, 0), ("o", 3, 0), ("att", 0, 0),
    ("mid", 3, 0), ("share", 0, 0), ("o", 3, 2), ("q2", 1, 0), ("att", 1, 0), ("share", 1, 0),
    ("pre", 1, 0), ("o", 3, 1), ("q2", 2, 0), ("att", 2, 0), ("share", 2, 0), ("pre", 2, 0),
    ("pre", 0, 0), ("fin", 2, 0), ("fin", 1, 0), ("pre", 3, 0), ("fin", 0, 0), ("fin", 3, 0),
)
ORDER_INNER = (
    ("owno", 2, 0), ("owno", 1, 0), ("own", 0, 0), ("o", 1, 1), ("o", 2, 0), ("o", 0, 1),
    ("owno", 0, 0), ("o", 1, 0), ("w", 0, 0), ("w", 0, 1), ("o", 2, 1), ("tf", 0, 0), ("o", 0, 2),
    ("o", 0, 0), ("o", 1, 2), ("w", 1, 1), ("w", 0, 2), ("own", 2, 0), ("o", 2, 2), ("w", 2, 1),
    ("t", 0, 0), ("ocy", 0, 1), ("own", 1, 0), ("ocy", 1, 1), ("o", 3, 1), ("ocx", 0, 0),
    ("w", 1, 2), ("kv1", 0, 0), ("w", 1, 0), ("ocx", 0, 1), ("w", 2, 0), ("ocx", 0, 2),
    ("w", 2, 2), ("ocx", 1, 1), ("own", 3, 0), ("ocy", 1, 2), ("q1", 1, 0), ("w", 3, 1),
    ("q1", 0, 0), ("w", 3, 2), ("w", 3, 0), ("ocy", 0, 2), ("ocy", 2, 2), ("mid", 0, 0),
    ("owno", 3, 0), ("ocx", 1, 2), ("q1", 2, 0), ("mid", 1, 0), ("kv2", 0, 0), ("mid", 2, 0),
    ("mid", 3, 0), ("ocx", 2, 1), ("o", 3, 2), ("o", 3, 0), ("q2", 1, 0), ("q2", 0, 0),
    ("ocy", 2, 0), ("q2", 2, 0), ("ocx", 1, 0), ("ocy", 0, 0), ("att", 0, 0), ("ocy", 1, 0),
    ("ocx", 2, 2), ("ocy", 2, 1), ("share", 0, 0), ("att", 1, 0), ("ocx", 2, 0), ("att", 2, 0),
    ("pre", 3, 0), ("share", 2, 0), ("share", 1, 0), ("pre", 0, 0), ("pre", 1, 0), ("fin", 1, 0),
    ("pre", 2, 0), ("fin", 0, 0), ("fin", 2, 0), ("fin", 3, 0),
)


def pick(at, values):
    out = jnp.int32(values[0])
    for i, v in enumerate(values[1:]):
        out = jnp.where(at == i + 1, jnp.int32(v), out)
    return out


class Run:
    def __init__(self, ends):
        self.ends = ends
        self.shared = 0
        self.whole = set()
        self.projected = False
        self.sent = collections.defaultdict(int)

    def begin(self, c, kind, ref):
        c.start()
        self.sent[kind] += math.prod(ref.shape)


def kernel(
    n, tokens, query_w, key_w, value_w, out_w, listing, live_in, mixed,
    tok, other, crossing, held, weights, outs, lists, table, picked, mine, passing, away, back, away_on, back_on,
    queries, bias, attended, summed, chosen, live, local_sem, send_sem, recv_sem,
):
    dp, me, tp = lax.axis_index("dp"), lax.axis_index("kv"), lax.axis_index("tp")
    x_at, y_at = lax.rem(dp, 2), lax.div(dp, 2)
    right, left = jnp.minimum(me + 1, n - 1), jnp.maximum(me - 1, 0)
    to_x = {"dp": 2 * y_at + (1 - x_at)}
    to_y = {"dp": 2 * (1 - y_at) + x_at}
    dp_x, dp_y = 2 * y_at + (1 - x_at), 2 * (1 - y_at) + x_at
    dp_far = 2 * (1 - y_at) + (1 - x_at)
    side = lax.rem(x_at + y_at, 2)
    partner = {"tp": 1 - tp}
    to_far = {"dp": 2 * (1 - y_at) + (1 - x_at)}
    rows = tok.shape[0]
    depth = weights[0].shape[0]
    per_dev = rows // BLOCK
    seg = depth // n
    parts = 4
    groups, chunks = len(weights), len(outs)
    widths = [ref.shape[1] for ref in weights]
    firsts = [sum(widths[1:g]) for g in range(groups)]
    starts = [sum(widths[:g]) for g in range(groups)]
    tiles = [ref.shape[1] for ref in outs]
    owned = outs[0].shape[0] // n
    is_end = jnp.logical_or(me == 0, me == n - 1)
    inward = {"kv": jnp.where(me == 0, right, left)}
    near = [pick(me, v) for v in ((1, 2, 1, 2), (2, 0, 3, 1), (3, 3, 0, 0))]

    def load(src, dst, at):
        c = pltpu.make_async_copy(src, dst, local_sem.at[at])
        c.start()

    def loaded(ref, at):
        pltpu.make_async_copy(ref, ref, local_sem.at[at]).wait()

    def remote(src, dst, send, recv, target):
        return pltpu.make_async_remote_copy(
            src_ref=src, dst_ref=dst, send_sem=send_sem.at[send], recv_sem=recv_sem.at[recv],
            device_id=target, device_id_type=MESH,
        )

    def arrived(ref, recv):
        remote(ref, ref, 0, recv, partner).wait_recv()

    barrier = pltpu.get_barrier_semaphore()

    def greet(target):
        pl.semaphore_signal(barrier, inc=1, device_id=target, device_id_type=MESH)

    pl.when(me < n - 1)(lambda: greet({"kv": right}))
    pl.when(me > 0)(lambda: greet({"kv": left}))
    for target in (to_x, to_y, partner):
        greet(target)

    for s in range(chunks):
        load(
            out_w.at[:, sum(tiles[:s]) : sum(tiles[: s + 1])],
            outs[s].at[pl.ds(pl.multiple_of(me * owned, owned), owned), :],
            groups + s,
        )
    load(key_w, held[0].at[:, :HD], 0)
    load(value_w, held[0].at[:, HD:], 0)
    for g in range(1, groups):
        load(query_w.at[:, firsts[g] : firsts[g] + widths[g]], held[g], g)
    load(listing, lists.at[me], groups + chunks)
    load(listing, chosen, groups + chunks + 1)
    load(live_in, live, groups + chunks + 2)
    def token_cols(owner, index, count):
        return pl.ds(pl.multiple_of((parts * owner + index) * seg, seg), count * seg)

    for i, owner in enumerate(near):
        load(
            tokens.at[:, token_cols(owner, dp, 1)], tok.at[:, i * seg : (i + 1) * seg],
            groups + chunks + 3,
        )
    load(
        tokens.at[:, token_cols(me, 0, parts)], tok.at[:, (n - 1) * seg :], groups + chunks + 3
    )

    with jax.named_scope("barrier"):
        pl.semaphore_wait(barrier, jnp.where(is_end, 4, 5))

    others = n - 1
    W = 0
    O = W + groups * others
    OX = O + chunks * others
    OY = OX + chunks * others
    OC = OY + chunks * others
    T = OC + chunks
    L = T + 4
    K = L + others
    Y = K + others
    S = Y + 2 * groups
    REST = groups + chunks
    LATE, CROSS, FORTH, TOKENS, LISTS = (REST + 1 + i for i in range(5))
    BLOCKS = LISTS + others

    def from_owner(owner, receiver):
        return lax.rem(owner + n - receiver, n) - 1

    my_part = pl.ds(pl.multiple_of(tp * (rows // 2), rows // 2), rows // 2)
    their_part = pl.ds(pl.multiple_of((1 - tp) * (rows // 2), rows // 2), rows // 2)
    few = rows // 4
    first_rows = [pl.ds(pl.multiple_of(tp * (rows // 2) + i * few, few), few) for i in range(2)]

    def t_send(part, target, to, recv, via):
        for i, owner in enumerate(near):
            remote(
                tokens.at[part, token_cols(owner, target["dp"], 1)],
                to.at[:, i * seg : (i + 1) * seg], TOKENS, recv, via,
            ).start()

    t_send(my_part, to_x, other.at[0, my_part], T, to_x)
    t_send(my_part, to_y, other.at[1, my_part], T, to_y)
    t_send(first_rows[0], to_far, crossing.at[0], T + 2, to_x)
    t_send(first_rows[1], to_far, crossing.at[1], T + 3, to_y)

    def t_cross(run):
        for i, target in enumerate((to_y, to_x)):
            piece = crossing.at[i]
            arrived(piece, T + 2 + i)
            run.begin(
                remote(piece, other.at[2, first_rows[i]], CROSS, T, target), CROSS, piece
            )

    def t_share(run):
        piece = other.at[:, my_part, :]
        arrived(piece, T)
        run.begin(remote(piece, piece, FORTH, T + 1, partner), FORTH, piece)

    def l_copy(step):
        return remote(
            listing, lists.at[me], LISTS + step - 1, L + step - 1, {"kv": jnp.maximum(me - step, 0)}
        )

    pl.when(me >= 1)(l_copy(1).start)

    def z_targets(run):
        return [inward] if run.ends else [{"kv": right}, {"kv": left}]

    def w_piece(group, owner):
        return weights[group].at[pl.ds(pl.multiple_of(owner * seg, seg), seg), :]

    def w_own(run, group):
        loaded(held[group], group)
        source = held[group].at[pl.ds(pl.multiple_of(dp * seg, seg), seg), :]
        piece = w_piece(group, me)
        for target in z_targets(run):
            recv = W + group * others + from_owner(me, target["kv"])
            run.begin(remote(source, piece, group, recv, target), group, source)

    def w_step(run, group, slot):
        owner = near[slot]
        piece = w_piece(group, owner)
        arrived(piece, W + group * others + from_owner(owner, me))
        if not run.ends:
            to = jnp.where(owner < me, right, left)
            recv = W + group * others + from_owner(owner, to)
            run.begin(remote(piece, piece, group, recv, {"kv": to}), group, piece)

    quarter = owned // 4

    def o_piece(s, owner, first, size):
        return outs[s].at[pl.ds(pl.multiple_of(owner * owned + first, LEAST), size), :]

    def o_send(run, s, piece, recv, target):
        kind = groups + s
        run.begin(remote(piece, piece, kind, recv, target), kind, piece)

    def carried(s, owner):
        if MODES[s] in CUTS:
            return o_piece(s, owner, dp * quarter, quarter)
        return o_piece(s, owner, side * 2 * quarter, 2 * quarter)

    def o_own(run, s):
        loaded(outs[s].at[:owned, :], groups + s)
        for target in z_targets(run):
            o_send(run, s, carried(s, me), O + s * others + from_owner(me, target["kv"]), target)

    def o_step(run, s, slot):
        owner = near[slot]
        piece = carried(s, owner)
        arrived(piece, O + s * others + from_owner(owner, me))
        if not run.ends:
            to = jnp.where(owner < me, right, left)
            o_send(run, s, piece, O + s * others + from_owner(owner, to), {"kv": to})
        if MODES[s] in CUTS:
            at = s * others + from_owner(owner, me)
            o_send(run, s, piece, OX + at, to_x)
            o_send(run, s, piece, OY + at, to_y)
        else:
            o_send(run, s, o_piece(s, owner, 2 * side * quarter, quarter), OC + s, to_x)
            o_send(run, s, o_piece(s, owner, (2 * side + 1) * quarter, quarter), OC + s, to_y)

    def o_turn(run, s, slot, along_x):
        owner, cut = near[slot], CUTS[MODES[s]]
        at = s * others + from_owner(owner, me)
        if along_x:
            arrived(o_piece(s, owner, dp_x * quarter, quarter), OX + at)
            if cut:
                o_send(run, s, o_piece(s, owner, dp_x * quarter, cut), OC + s, to_y)
        else:
            arrived(o_piece(s, owner, dp_y * quarter, quarter), OY + at)
            o_send(run, s, o_piece(s, owner, dp_y * quarter + cut, quarter - cut), OC + s, to_x)

    def o_arrive(s):
        count = 1 if MODES[s] in CUTS else 2
        arrived(outs[s].at[: others * count * quarter, :], OC + s)

    def part(source, group):
        out = jnp.zeros((rows, widths[group]), jnp.float32)
        for i, owner in enumerate(near):
            slab = pl.ds(pl.multiple_of(owner * seg, seg), seg)
            out += jnp.dot(
                source[:, i * seg : (i + 1) * seg], weights[group][slab, :],
                preferred_element_type=jnp.float32,
            )
        return out

    def columns(group):
        return slice(starts[group], starts[group] + widths[group])

    def y_copy(group, along_y):
        return remote(
            away[along_y].at[:, columns(group)], back[along_y].at[:, columns(group)], REST,
            Y + 2 * group, to_y if along_y else to_x,
        )

    def on_copy(group, along_y):
        return remote(
            away_on[along_y].at[:, columns(group)], back_on[along_y].at[:, columns(group)], LATE,
            Y + 2 * group + 1, to_y if along_y else to_x,
        )

    def project(run, group):
        if not run.projected:
            arrived(other.at[:, their_part, :], T + 1)
            run.projected = True
        cols, half = columns(group), rows // 2
        far = part(other.at[2], group).astype(jnp.bfloat16)
        beside = part(other.at[0], group)
        above = part(other.at[1], group)
        away[0][:half, cols] = beside[:half].astype(jnp.bfloat16)
        away[0][half:, cols] = far[:half]
        away[1][:half, cols] = above[half:].astype(jnp.bfloat16)
        away[1][half:, cols] = far[half:]
        for along_y in range(2):
            run.begin(y_copy(group, along_y), REST, away[along_y].at[:, cols])
        passing[1, :, cols] = above[:half]
        passing[0, :, cols] = beside[half:]
        mine[:, cols] = part(tok, group) + jnp.dot(
            tok[:, (n - 1) * seg :], held[group][...], preferred_element_type=jnp.float32
        )

    def pass_on(run, group):
        cols, half = columns(group), rows // 2
        arrived(tok.at[:, : 2 * widths[group]], Y + 2 * group)
        for along_y in (1, 0):
            took = back[1 - along_y][half:, cols].astype(jnp.float32)
            away_on[along_y][:, cols] = (passing[along_y, :, cols] + took).astype(jnp.bfloat16)
            run.begin(on_copy(group, along_y), LATE, away_on[along_y].at[:, cols])

    def collected(group):
        cols, half = columns(group), rows // 2
        arrived(tok.at[:, : widths[group]], Y + 2 * group + 1)
        halves = []
        for i, along_y in enumerate((1, 0)):
            halves.append(
                mine[i * half : (i + 1) * half, cols]
                + back[1 - along_y][:half, cols].astype(jnp.float32)
                + back_on[along_y][:, cols].astype(jnp.float32)
            )
        return jnp.concatenate(halves, axis=0).astype(jnp.bfloat16)

    slots = CAP * BLOCK
    local_at = n * slots

    def found(listed, block):
        return jnp.max((listed == block).astype(jnp.float32), axis=(0, 1), keepdims=True)

    def marks(listed, first):
        rank = jnp.zeros((1, 1), jnp.float32)
        out = [[] for _ in range(CAP)]
        for b in range(per_dev):
            one = found(listed, first + b)
            rank = rank + one
            for s in range(CAP):
                out[s].append(jnp.where(rank == s + 1, one, 0.0))
        return out

    def k_copy(step):
        return remote(
            picked.at[step - 1], table.at[pl.ds(pl.multiple_of(me * slots, slots), slots), :],
            BLOCKS + step - 1, K + step - 1, {"kv": jnp.minimum(me + step, n - 1)},
        )

    def k_arrive():
        for step in range(1, n):
            pl.when(me >= step)(k_copy(step).wait_recv)

    def share_blocks(run):
        full = collected(0)
        table[local_at : local_at + rows, :] = full
        full = full.astype(jnp.float32)
        for step in range(1, n):
            pl.when(me + step < n)(l_copy(step).wait_recv)
        for step in range(1, n):

            def send_to(step=step):
                which = marks(lists[me + step], me * per_dev)
                for s in range(CAP):
                    kept = jnp.zeros((BLOCK, full.shape[1]), jnp.float32)
                    for b in range(per_dev):
                        kept = kept + which[s][b] * full[b * BLOCK : (b + 1) * BLOCK, :]
                    picked[step - 1, s * BLOCK : (s + 1) * BLOCK, :] = kept.astype(jnp.bfloat16)

            pl.when(me + step < n)(send_to)
            pl.when(me + step < n)(k_copy(step).start)

    def build_bias():
        loaded(lists.at[me], groups + chunks)
        loaded(chosen, groups + chunks + 1)
        loaded(live, groups + chunks + 2)
        listed = lists[me]
        seq = bias.shape[1]
        column = lax.broadcasted_iota(jnp.int32, (8, seq), 1)
        block = me * per_dev + lax.div(column - local_at, BLOCK)
        for owner in range(n):
            which = marks(listed, owner * per_dev)
            for s in range(CAP):
                ident = jnp.full((1, 1), -2.0, jnp.float32)
                for b in range(per_dev):
                    ident = jnp.where(which[s][b] > 0.5, float(owner * per_dev + b), ident)
                ident = jnp.where(me == owner, -2.0, ident).astype(jnp.int32)
                block = jnp.where(lax.div(column, BLOCK) == owner * CAP + s, ident, block)
        at = block * BLOCK + lax.rem(column, BLOCK)
        at = jnp.concatenate([at] * (BLOCK // 8), axis=0)
        row = lax.broadcasted_iota(jnp.int32, (BLOCK, seq), 0)
        for j in range(per_dev):
            open_to = jnp.full((8, seq), -jnp.inf, jnp.float32)
            for e in range(chosen.shape[1]):
                open_to = jnp.where(block == chosen[j, e], 0.0, open_to)
            spread = jnp.concatenate([open_to] * (BLOCK // 8), axis=0)
            causal = at <= row + (me * rows + j * BLOCK)
            bias[j * BLOCK : (j + 1) * BLOCK, :] = jnp.where(causal, spread, -jnp.inf)

    def queries_done(group):
        queries[:, firsts[group] : firsts[group] + widths[group]] = collected(group)

    def attend(group):
        if group == 1:
            k_arrive()
        alive = me * rows + lax.broadcasted_iota(jnp.int32, (rows, HD), 0) < live[0]
        for h in range(firsts[group] // HD, (firsts[group] + widths[group]) // HD):
            cols = slice(h * HD, (h + 1) * HD)
            scores = lax.dot_general(
                queries[:, cols], table[:, :HD], (((1,), (1,)), ((), ())),
                preferred_element_type=jnp.float32,
            )
            masked = scores * HD ** (-0.5) + bias[...]
            top = jnp.max(masked, axis=1, keepdims=True)
            probs = jnp.exp(masked - top)
            total = jnp.sum(probs, axis=1, keepdims=True)
            summed = jnp.dot(
                probs.astype(jnp.bfloat16), table[:, HD:], preferred_element_type=jnp.float32
            )
            attended[tp, :, cols] = jnp.where(alive, summed / total, 0.0).astype(jnp.bfloat16)

    def of_group(which, group):
        return attended.at[which, :, firsts[group] : firsts[group] + widths[group]]

    def share(run, group):
        piece = of_group(tp, group)
        run.begin(remote(piece, piece, LATE, S + group - 1, partner), LATE, piece)

    def shared(run, last):
        while run.shared < last:
            run.shared += 1
            arrived(of_group(1 - tp, run.shared), S + run.shared - 1)

    wide = queries.shape[1]

    def mix(s, first, last):
        acc = jnp.zeros((rows, tiles[s]), jnp.float32)
        for which in range(2):
            acc += jnp.dot(
                attended[which, :, first:last],
                outs[s][which * wide + first : which * wide + last, :],
                preferred_element_type=jnp.float32,
            )
        return acc

    def early(run, s):
        shared(run, 1)
        o_arrive(s)
        summed[:, sum(tiles[:s]) : sum(tiles[: s + 1])] = mix(s, 0, widths[1])

    def final(run, s):
        shared(run, groups - 1)
        cols = slice(sum(tiles[:s]), sum(tiles[: s + 1]))
        if s in run.whole:
            o_arrive(s)
            mixed[:, cols] = mix(s, 0, wide).astype(jnp.bfloat16)
        else:
            mixed[:, cols] = (summed[:, cols] + mix(s, widths[1], wide)).astype(jnp.bfloat16)

    def settle():
        for owner in range(n):

            def clear(owner=owner):
                table[owner * slots : (owner + 1) * slots, :] = jnp.zeros(
                    (slots, table.shape[1]), table.dtype
                )

            pl.when(owner >= me)(clear)
        build_bias()
        loaded(tok, groups + chunks + 3)

    def act(run, name, i, j):
        if name == "own":
            w_own(run, i)
        elif name == "owno":
            o_own(run, i)
        elif name == "t":
            t_share(run)
        elif name == "tf":
            t_cross(run)
        elif name == "w":
            w_step(run, i, j)
        elif name == "o":
            o_step(run, i, j)
        elif name == "ocx" or name == "ocy":
            o_turn(run, i, j, name == "ocx")
        elif name == "kv1":
            for step in range(2, n):
                pl.when(me >= step)(l_copy(step).start)
            project(run, 0)
        elif name == "mid":
            pass_on(run, i)
        elif name == "kv2":
            share_blocks(run)
        elif name == "q1":
            project(run, 1 + i)
        elif name == "q2":
            queries_done(1 + i)
        elif name == "att":
            attend(1 + i)
        elif name == "share":
            share(run, 1 + i)
        elif name == "pre":
            early(run, i)
        else:
            final(run, i)

    def follow(order, ends):
        run = Run(ends)
        begun = False
        for at, (name, i, j) in enumerate(order):
            if name == "pre" and order[at + 1] == ("fin", i, j):
                run.whole.add(i)
                continue
            if not begun and not name.startswith("own"):
                settle()
                begun = True
            with jax.named_scope(f"{name}_{i}_{j}"):
                act(run, name, i, j)
        for kind, size in run.sent.items():
            if groups <= kind < groups + chunks:
                ref = outs[kind - groups].at[: size // tiles[kind - groups], :]
            elif kind < groups or kind in (REST, LATE):
                ref = tok.at[:, : size // rows]
            elif kind == CROSS:
                ref = crossing
            else:
                ref = other.at[:, my_part, :]
            remote(ref, ref, kind, 0, partner).wait_send()

    pl.when(is_end)(functools.partial(follow, ORDER_END, True))
    pl.when(jnp.logical_not(is_end))(functools.partial(follow, ORDER_INNER, False))
    ref = other.at[:, my_part, :]
    remote(ref, ref, TOKENS, T, to_x).wait_send()
    for step in range(1, n):
        pl.when(me >= step)(l_copy(step).wait_send)
        pl.when(me + step < n)(k_copy(step).wait_send)


def woven_body(tokens, query_weight, key_weight, value_weight, out_weight, chosen, live_length):
    n = lax.axis_size("kv")
    rows, model = tokens.shape
    wide = query_weight.shape[1]
    seg = model // n // 4
    width = 2 * HD
    widths = [width] + [heads * HD for heads in HEADS]
    unit = out_weight.shape[1] // sum(SHARES)
    tiles = [share * unit for share in SHARES]
    groups, chunks = len(widths), len(tiles)
    every = sum(widths)
    slots = CAP * BLOCK
    total = n * slots + rows
    dma = pltpu.SemaphoreType.DMA
    bf16 = jnp.bfloat16
    f32 = jnp.float32
    anywhere = pl.BlockSpec(memory_space=pl.ANY)
    others = n - 1
    arrivals = groups * (others + 2) + chunks * (3 * others + 1) + 4 + 2 * others + groups - 1
    return pl.pallas_call(
        functools.partial(kernel, n),
        out_shape=pltpu.VMEM((rows, out_weight.shape[1]), bf16),
        in_specs=[anywhere] * 7,
        out_specs=pl.BlockSpec(memory_space=pltpu.VMEM),
        scratch_shapes=[
            pltpu.VMEM((rows, (n - 1) * seg + model // n), bf16),
            pltpu.VMEM((3, rows, (n - 1) * seg), bf16),
            pltpu.VMEM((2, rows // 4, (n - 1) * seg), bf16),
            tuple(pltpu.VMEM((key_weight.shape[0], w), bf16) for w in widths),
            tuple(pltpu.VMEM((n * seg, w), bf16) for w in widths),
            tuple(pltpu.VMEM((n * out_weight.shape[0], w), bf16) for w in tiles),
            pltpu.VMEM((n,) + chosen.shape, jnp.int32),
            pltpu.VMEM((total, width), bf16),
            pltpu.VMEM((n - 1, slots, width), bf16),
            pltpu.VMEM((rows, every), f32),
            pltpu.VMEM((2, rows // 2, every), f32),
            tuple(pltpu.VMEM((rows, every), bf16) for _ in range(2)),
            tuple(pltpu.VMEM((rows, every), bf16) for _ in range(2)),
            tuple(pltpu.VMEM((rows // 2, every), bf16) for _ in range(2)),
            tuple(pltpu.VMEM((rows // 2, every), bf16) for _ in range(2)),
            pltpu.VMEM((rows, wide), bf16),
            pltpu.VMEM((rows, total), f32),
            pltpu.VMEM((2, rows, wide), bf16),
            pltpu.VMEM((rows, out_weight.shape[1]), f32),
            pltpu.SMEM(chosen.shape, jnp.int32),
            pltpu.SMEM(live_length.shape, jnp.int32),
            dma((groups + chunks + 4,)),
            dma((groups + chunks + 5 + 2 * others,)),
            dma((arrivals,)),
        ],
        compiler_params=pltpu.CompilerParams(
            collective_id=0, has_side_effects=True, vmem_limit_bytes=56 * 2**20
        ),
    )(tokens, query_weight, key_weight, value_weight, out_weight, chosen, live_length)


def solution(mesh):
    in_specs = (
        P(("dp", "kv"), None),
        P("kv", "tp"),
        P("kv", "tp"),
        P("kv", "tp"),
        P("kv", "tp"),
        P(("dp", "kv"), None),
        P("dp"),
    )
    out_specs = P(("dp", "kv"), "tp")
    fits = (mesh.shape["dp"], mesh.shape["kv"], mesh.shape["tp"]) == (4, 4, 2)
    body = woven_body if fits else gathered_body
    return jax.shard_map(body, mesh=mesh, in_specs=in_specs, out_specs=out_specs, check_vma=False)
```
